32 devices in a mesh: sp: 8 (over z, y), tp: 4 (over x, core).
Axes of the slice: x: 2, y: 2, z: 4, core: 2. Of those that a mesh axis runs over, the one named last changes fastest.
Arguments:
- tokens: bfloat16 [1536, 2048], P('sp'), may hold values from -10 to 10
- w_query: bfloat16 [2048, 1024], P(None, 'tp'), may hold values from -0.125 to 0.125
- w_key: bfloat16 [2048, 256], P(None, 'tp'), may hold values from -0.125 to 0.125
- w_value: bfloat16 [2048, 256], P(None, 'tp'), may hold values from -0.125 to 0.125
- w_output: bfloat16 [1024, 2048], P('tp'), may hold values from -0.1875 to 0.1875
- query_gain: float32 [64], replicated, may hold values from 0.4 to 9
- key_gain: float32 [64], replicated, may hold values from 0.4 to 9
Outputs:
- mixed_out: bfloat16 [1536, 2048], P(('sp', 'tp'))
- log_sums: float32 [16, 1536], P('tp', 'sp')
The draws below stay inside these ranges and needn't reach their ends.
All inputs are finite; a program needn't handle non-finite values.
Results may differ from the reference program's by a relative error of at most 0.009.
The reference program's roundings to bfloat16 on the way (of `weights` and `attended`) count: a program that leaves them out, or rounds other values in their place, can miss the bound.
Values may be sent and summed in bfloat16 or wider, within the bound.
No kernel may reach another device: no remote copies, remote signals or barrier semaphores. Data moves between devices by JAX's collectives and lax.ppermute only.
A program may use at most 64 MiB of HBM per device.

```python
import math
import jax
import jax.numpy as jnp
from jax import lax

D = 2048
HEADS = 16
KV_HEADS = 4
HEAD = 64
GRID_W = 64
TOK_DEV = 192
TOKENS = 1536


def draw_tokens(key, part):
    first, second, third = jax.random.split(key, 3)
    n_blocks = TOKENS // TOK_DEV
    base = jax.random.normal(first, (TOKENS, D), jnp.float32)
    offsets = jax.random.uniform(second, (n_blocks, 1), jnp.float32, -0.5, 2.0)
    direction = jnp.clip(jax.random.normal(third, (1, D), jnp.float32), -3.0, 3.0)
    shifted = base + jnp.repeat(offsets, TOK_DEV, axis=0) * direction
    return jnp.clip(shifted, -10.0, 10.0).astype(jnp.bfloat16)


def gain_draw(key, salt):
    own = jax.random.fold_in(key, salt)
    base = 1.0 + 0.18 * jnp.clip(jax.random.normal(own, (HEAD,), jnp.float32), -3.0, 3.0)
    return base


def draw_query_gain(key, part):
    return gain_draw(key, 11)


def draw_key_gain(key, part):
    return gain_draw(key, 13)


def steps_of(stream_key, extent, cuts, smallest, largest):
    loudness = 1.0
    for dim, blocks in cuts:
        draws = jax.random.uniform(jax.random.fold_in(jax.random.fold_in(stream_key, 6), dim), (blocks,), jnp.float32, smallest / len(cuts), largest / len(cuts))
        loudness = loudness * jnp.repeat(jnp.exp(draws), extent[dim] // blocks).reshape((-1,) + (1,) * (len(extent) - 1 - dim))
    return loudness


def centred(stream_key, shape, spread, limit, cuts=(), held_as=jnp.bfloat16):
    factor_of = steps_of(stream_key, shape, cuts, -0.22, 0.18) if cuts else 1.0
    drawn = jax.random.normal(stream_key, shape, jnp.float32) * spread * factor_of
    return jnp.minimum(jnp.maximum(drawn, -limit), limit).astype(held_as)


def setup_inputs(seed: int = 0) -> dict:
    splits = jax.random.split(jax.random.key(seed), 8)
    tokens = draw_tokens(jax.random.fold_in(splits[7], 71), 0)
    w_query = centred(splits[1], (D, HEADS * HEAD), D ** -0.5, 0.125, ((1, 4),))
    w_key = centred(splits[2], (D, KV_HEADS * HEAD), D ** -0.5, 0.125, ((1, 4),))
    w_value = centred(splits[3], (D, KV_HEADS * HEAD), D ** -0.5, 0.125, ((1, 4),))
    w_output = centred(splits[4], (HEADS * HEAD, D), (HEADS * HEAD) ** -0.5, 0.1875, ((0, 4),))
    query_gain = draw_query_gain(jax.random.fold_in(splits[7], 71), 0)
    key_gain = draw_key_gain(jax.random.fold_in(splits[7], 71), 0)
    return dict(tokens=tokens, w_query=w_query, w_key=w_key, w_value=w_value, w_output=w_output, query_gain=query_gain, key_gain=key_gain)


ROPE_BASE = 10000.0
NORM_EPS = 1e-06

def rotate(values, position):
    dim = values.shape[-1]
    half_dim = dim // 2
    inverse = ROPE_BASE ** (-jnp.arange(half_dim, dtype=jnp.float32) * (2.0 / dim))
    angles = position.astype(jnp.float32)[:, None] * inverse[None, :]
    cosine = jnp.cos(angles)[:, None, :]
    sine = jnp.sin(angles)[:, None, :]
    first_half = values[..., :half_dim]
    second_half = values[..., half_dim:]
    return jnp.concatenate([first_half * cosine - second_half * sine, second_half * cosine + first_half * sine], -1)

def prepare(projected, gain_vec, grid_row, grid_col):
    values = projected.astype(jnp.float32)
    values = values * lax.rsqrt(lax.optimization_barrier(jnp.mean(values * values, -1, keepdims=True)) + NORM_EPS) * gain_vec
    split_at = values.shape[-1] // 2
    turned = jnp.concatenate([rotate(values[..., :split_at], grid_row), rotate(values[..., split_at:], grid_col)], -1)
    return turned.astype(jnp.bfloat16)

def reference(tokens, w_query, w_key, w_value, w_output, query_gain, key_gain):
    seq_len = tokens.shape[0]
    head_dim = query_gain.shape[0]
    query_raw = jnp.dot(tokens, w_query, preferred_element_type=jnp.float32).astype(jnp.bfloat16)
    key_raw = jnp.dot(tokens, w_key, preferred_element_type=jnp.float32).astype(jnp.bfloat16)
    value_raw = jnp.dot(tokens, w_value, preferred_element_type=jnp.float32).astype(jnp.bfloat16)
    positions = jnp.arange(seq_len, dtype=jnp.int32)
    grid_row = positions // GRID_W
    grid_col = positions % GRID_W
    queries = prepare(query_raw.reshape(seq_len, HEADS, head_dim), query_gain, grid_row, grid_col)
    key_rows = prepare(key_raw.reshape(seq_len, KV_HEADS, head_dim), key_gain, grid_row, grid_col)
    value_rows = value_raw.reshape(seq_len, KV_HEADS, head_dim).astype(jnp.float32)
    key_float = key_rows.astype(jnp.float32)
    group_size = HEADS // KV_HEADS
    block_len = math.gcd(seq_len, 256)
    n_blocks = seq_len // block_len
    query_blocks = queries.reshape(n_blocks, block_len, KV_HEADS, group_size, head_dim)
    score_scale = head_dim ** (-0.5)

    def one_block(query_block):
        scores = jnp.einsum('qkgd,skd->kgqs', query_block.astype(jnp.float32), key_float) * score_scale
        row_max = lax.optimization_barrier(jnp.max(scores, -1))
        expos = jnp.exp(scores - row_max[..., None])
        weight_sum = lax.optimization_barrier(jnp.sum(expos, -1))
        weights = expos.astype(jnp.bfloat16).astype(jnp.float32)
        summed = jnp.einsum('kgqs,skd->qkgd', weights, value_rows)
        summed = summed / jnp.transpose(weight_sum, (2, 0, 1))[..., None]
        attended_block = summed.astype(jnp.bfloat16).reshape(block_len, HEADS * head_dim)
        log_block = (row_max + jnp.log(weight_sum)).reshape(HEADS, block_len)
        return (attended_block, log_block)
    attended_all, log_all = lax.map(one_block, query_blocks)
    attended = attended_all.reshape(seq_len, HEADS * head_dim)
    log_sums = jnp.transpose(log_all, (1, 0, 2)).reshape(HEADS, seq_len)
    mixed_out = jnp.dot(attended, w_output, preferred_element_type=jnp.float32).astype(jnp.bfloat16)
    return (mixed_out, log_sums)
```

```python
import functools

import jax
import jax.numpy as jnp
import numpy as np
from jax import lax
from jax.experimental import pallas as pl
from jax.experimental.pallas import tpu as pltpu
from jax.sharding import PartitionSpec as P

GRID_W = 64
ROPE_BASE = 10000.0
NORM_EPS = 1e-06
LANES = 128
NEG = -1e30


VMEM = pl.BlockSpec(memory_space=pltpu.VMEM)
NT = (((1,), (1,)), ((), ()))


def rope_tables(n_rows, head_dim):
    half = head_dim // 2
    quarter = half // 2
    inverse = ROPE_BASE ** (-np.arange(quarter, dtype=np.float64) * (2.0 / half))
    channel = np.arange(LANES) % head_dim
    freq = inverse[channel % quarter]
    sign = np.where(channel % half < quarter, -1.0, 1.0)
    by_row = channel < half

    def table(count, lanes):
        angles = np.arange(count, dtype=np.float64)[:, None] * freq[None, :]
        cosine = np.where(lanes[None, :], np.cos(angles), 0.0)
        sine = np.where(lanes[None, :], np.sin(angles) * sign[None, :], 0.0)
        return np.concatenate([cosine, sine], axis=1)

    pad = -n_rows % 8
    rows = np.concatenate([table(n_rows, by_row), np.zeros((pad, 2 * LANES))])
    return np.concatenate([table(GRID_W, ~by_row), rows]).astype(np.float32)


def turn(values, row_start, table_ref, head_dim):
    quarter = head_dim // 4
    rows = values.shape[0]
    lane = lax.broadcasted_iota(jnp.int32, (1, LANES), 1)
    ahead = pltpu.roll(values, LANES - quarter, 1)
    behind = pltpu.roll(values, quarter, 1)
    other = jnp.where(lane % (2 * quarter) < quarter, ahead, behind)
    columns = table_ref[0:GRID_W, :]
    out = []
    for j in range(rows // GRID_W):
        row = table_ref[pl.ds(GRID_W + row_start + j, 1), :]
        both = columns + row
        part = slice(j * GRID_W, (j + 1) * GRID_W)
        out.append(values[part] * both[:, :LANES] + other[part] * both[:, LANES:])
    return jnp.concatenate(out, axis=0)


def normed(values, gain, head_dim):
    lane = lax.broadcasted_iota(jnp.int32, (1, LANES), 1)
    squares = values * values
    scale = jnp.zeros_like(values)
    for g in range(LANES // head_dim):
        mine = lane // head_dim == g
        mean = jnp.sum(jnp.where(mine, squares, 0.0), axis=1, keepdims=True) * (1.0 / head_dim)
        scale = jnp.where(mine, lax.rsqrt(mean + NORM_EPS), scale)
    return values * scale * gain


def kv_kernel(head_dim, tok_ref, wk_ref, wv_ref, gain_ref, table_ref, out_ref, both_ref):
    rows = tok_ref.shape[0]
    both_ref[0:head_dim, :] = wk_ref[...]
    both_ref[head_dim:, :] = wv_ref[...]
    raw = lax.dot_general(tok_ref[...], both_ref[...], NT, preferred_element_type=jnp.float32)
    raw = raw.astype(jnp.bfloat16).astype(jnp.float32)
    lane = lax.broadcasted_iota(jnp.int32, (1, LANES), 1)
    row_start = lax.axis_index("sp") * (rows // GRID_W)
    keys = turn(normed(raw, gain_ref[...], head_dim), row_start, table_ref, head_dim)
    out_ref[...] = jnp.where(lane < head_dim, keys, raw).astype(jnp.bfloat16)


def attend(q, kv, top, total, acc):
    scores = lax.dot_general(q, kv, NT, preferred_element_type=jnp.float32)
    new_top = jnp.max(scores, axis=1, keepdims=True)
    if top is not None:
        new_top = jnp.maximum(top, new_top)
    expos = jnp.exp(scores - new_top)
    part = expos[:, 0:LANES]
    for i in range(1, expos.shape[1] // LANES):
        part = part + expos[:, i * LANES : (i + 1) * LANES]
    rest = expos.shape[1] % LANES
    if rest:
        tail = expos[:, -rest:]
        part = part + jnp.concatenate(
            [tail, jnp.zeros((tail.shape[0], LANES - rest), jnp.float32)], axis=1
        )
    fresh = jnp.dot(expos.astype(jnp.bfloat16), kv, preferred_element_type=jnp.float32)
    if top is None:
        return new_top, part, fresh
    shrink = jnp.exp(top - new_top)
    return new_top, total * shrink + part, acc * shrink + fresh


def q_kernel(
    head_dim, tok_ref, wq_ref, gain_ref, table_ref, kv_ref, q_ref, top_ref, total_ref, acc_ref
):
    rows = tok_ref.shape[0]
    heads = wq_ref.shape[1] // head_dim
    raw = jnp.dot(tok_ref[...], wq_ref[...], preferred_element_type=jnp.float32)
    raw = raw.astype(jnp.bfloat16).astype(jnp.float32)
    lane = lax.broadcasted_iota(jnp.int32, (1, LANES), 1)
    row_start = lax.axis_index("sp") * (rows // GRID_W)
    per = LANES // head_dim
    for p in range(heads // per):
        x = raw[:, p * LANES : (p + 1) * LANES]
        y = turn(normed(x, gain_ref[...], head_dim), row_start, table_ref, head_dim)
        y = y * (head_dim ** -0.5)
        for g in range(per):
            z = y if g == 0 else pltpu.roll(y, LANES - g * head_dim, 1)
            h = p * per + g
            z = jnp.where(lane < head_dim, z, 0.0)
            q_ref[h * rows : (h + 1) * rows, :] = z.astype(jnp.bfloat16)
    for h in range(heads):
        part = slice(h * rows, (h + 1) * rows)
        top, total, acc = attend(q_ref[part, :], kv_ref[...], None, None, None)
        top_ref[part, :] = jnp.broadcast_to(top, (rows, LANES))
        total_ref[part, :] = total
        acc_ref[part, :] = acc


def chunked(length, limit):
    best = length
    while best > limit:
        best //= 2
    return best


def block_kernel(heads, n_kv, *refs):
    q_ref, kv_refs = refs[0], refs[1 : 1 + n_kv]
    top_in, total_in, acc_in, top_ref, total_ref, acc_ref = refs[1 + n_kv :]
    rows = q_ref.shape[0] // heads
    for h in range(heads):
        part = slice(h * rows, (h + 1) * rows)
        state = top_in[part, :][:, 0:1], total_in[part, :], acc_in[part, :]
        for kv_ref in kv_refs:
            length = kv_ref.shape[0]
            step = chunked(length, 512)
            if length == step:
                state = attend(q_ref[part, :], kv_ref[...], *state)
            else:

                def body(i, carry, kv_ref=kv_ref, step=step):
                    at = pl.multiple_of(i * step, step)
                    return attend(q_ref[part, :], kv_ref[pl.ds(at, step), :], *carry)

                state = lax.fori_loop(0, length // step, body, state)
        top, total, acc = state
        top_ref[part, :] = jnp.broadcast_to(top, (rows, LANES))
        total_ref[part, :] = total
        acc_ref[part, :] = acc


def finish_kernel(heads, head_dim, q_ref, kv_ref, top_in, total_in, acc_in, att_ref, log_ref):
    rows = q_ref.shape[0] // heads
    per = LANES // head_dim
    lane = lax.broadcasted_iota(jnp.int32, (1, LANES), 1)
    length = kv_ref.shape[0]
    step = chunked(length, 512)
    for p in range(heads // per):
        joined = None
        for g in range(per):
            h = p * per + g
            part = slice(h * rows, (h + 1) * rows)
            state = top_in[part, :][:, 0:1], total_in[part, :], acc_in[part, :]
            if length == step:
                state = attend(q_ref[part, :], kv_ref[...], *state)
            else:

                def body(i, carry):
                    at = pl.multiple_of(i * step, step)
                    return attend(q_ref[part, :], kv_ref[pl.ds(at, step), :], *carry)

                state = lax.fori_loop(0, length // step, body, state)
            top, total, acc = state
            summed = jnp.sum(total, axis=1, keepdims=True)
            log = jnp.broadcast_to(top + jnp.log(summed), (rows, LANES))
            at = 0
            while at < rows:
                size = min(LANES, rows - at)
                r = lax.broadcasted_iota(jnp.int32, (size, LANES), 0)
                c = lax.broadcasted_iota(jnp.int32, (size, LANES), 1)
                line = jnp.sum(jnp.where(r == c, log[at : at + size], 0.0), axis=0, keepdims=True)
                log_ref[h : h + 1, at : at + size] = line[:, :size]
                at += size
            out = acc / summed
            out = pltpu.roll(out, (LANES - head_dim + g * head_dim) % LANES, 1)
            out = jnp.where(lane // head_dim == g, out, 0.0)
            joined = out if joined is None else joined + out
        att_ref[:, p * LANES : (p + 1) * LANES] = joined.astype(jnp.bfloat16)


def call(kernel, out_shape, flops, n_in, **more):
    return pl.pallas_call(
        kernel,
        out_shape=out_shape,
        in_specs=[VMEM] * n_in,
        out_specs=jax.tree.map(lambda _: VMEM, out_shape),
        cost_estimate=pl.CostEstimate(flops=flops, bytes_accessed=flops // 256, transcendentals=0),
        **more,
    )


def shards(n_sp, n_tp, tokens, w_query, w_key, w_value, w_output, query_gain, key_gain):
    head_dim = query_gain.shape[0]
    rows, width = tokens.shape
    heads = w_query.shape[1] // head_dim
    per = LANES // head_dim
    table = jnp.asarray(rope_tables(n_sp * rows // GRID_W, head_dim))
    f32 = functools.partial(jax.ShapeDtypeStruct, dtype=jnp.float32)
    bf16 = functools.partial(jax.ShapeDtypeStruct, dtype=jnp.bfloat16)

    kv = call(
        functools.partial(kv_kernel, head_dim),
        bf16((rows, LANES)),
        2 * rows * width * LANES,
        5,
        scratch_shapes=[pltpu.VMEM((LANES, width), jnp.bfloat16)],
    )(tokens, w_key.T, w_value.T, jnp.tile(key_gain, per)[None, :], table)

    size = (heads * rows, LANES)
    state_shape = [f32(size)] * 3

    def q_and_own(kv):
        return call(
            functools.partial(q_kernel, head_dim),
            [bf16(size)] + state_shape,
            2 * rows * width * heads * head_dim,
            5,
        )(tokens, w_query, jnp.tile(query_gain, per)[None, :], table, kv)

    def blocks(q, kvs, state):
        return call(
            functools.partial(block_kernel, heads, len(kvs)),
            state_shape,
            sum(4 * size[0] * x.shape[0] * LANES for x in kvs),
            4 + len(kvs),
            input_output_aliases={1 + len(kvs) + i: i for i in range(3)},
        )(q, *kvs, *state)

    def xor(n, bit):
        return [(i, i ^ bit) for i in range(n)]

    held = kv
    q = state = None
    stride = 1
    pending = []
    while stride < n_sp:
        radix = 2 if stride == 1 else min(4, n_sp // stride)
        got = [
            lax.ppermute(held, "sp", xor(n_sp, d * stride)) for d in sorted(range(1, radix), reverse=True)
        ]
        if q is None:
            q, *state = q_and_own(kv)
        for x in pending:
            state = blocks(q, [x], state)
        pending = got[::-1]
        stride *= radix
        if stride < n_sp:
            held = jnp.concatenate([held] + got, axis=0)
    for x in pending[:-1]:
        state = blocks(q, [x], state)
    attended, log_sums = call(
        functools.partial(finish_kernel, heads, head_dim),
        [bf16((rows, heads * head_dim)), f32((heads, rows))],
        4 * size[0] * pending[-1].shape[0] * LANES,
        5,
    )(q, pending[-1], *state)

    own = rows // n_tp
    me = lax.axis_index("tp")

    def partial_out(block):
        part = lax.dynamic_slice_in_dim(attended, block * own, own, 0)
        return jnp.dot(part, w_output, preferred_element_type=jnp.float32)

    keep = {0: None}
    bits = []
    b = 1
    while b < n_tp:
        bits.append(b)
        b *= 2
    parts = {d: partial_out(me ^ d) for d in range(n_tp)}
    for b in bits:
        left = [d for d in parts if not d & b]
        sent = jnp.concatenate([parts[d ^ b].astype(jnp.bfloat16) for d in left], axis=0)
        got = lax.ppermute(sent, "tp", xor(n_tp, b)).astype(jnp.float32)
        parts = {d: parts[d] + got[i * own : (i + 1) * own] for i, d in enumerate(left)}
    return parts[0].astype(jnp.bfloat16), log_sums


def solution(mesh):
    placed = (P("sp", None), P(None, "tp"), P(None, "tp"), P(None, "tp"), P("tp", None), P(), P())
    return jax.shard_map(
        functools.partial(shards, mesh.shape["sp"], mesh.shape["tp"]),
        mesh=mesh,
        in_specs=placed,
        out_specs=(P(("sp", "tp"), None), P("tp", "sp")),
        check_vma=False,
    )
```

```python
import functools

import jax
import jax.numpy as jnp
import numpy as np
from jax import lax
from jax.experimental import pallas as pl
from jax.experimental.pallas import tpu as pltpu
from jax.sharding import PartitionSpec as P


GRID_W = 64
ROPE_BASE = 10000.0
NORM_EPS = 1e-06
LANES = 128
LIMIT = 12 << 20
KV_LIMIT = 56480000


VMEM = pl.BlockSpec(memory_space=pltpu.VMEM)
HBM = pl.BlockSpec(memory_space=pltpu.HBM)
NT = (((1,), (1,)), ((), ()))


def rope_tables(n_rows, head_dim):
    half = head_dim // 2
    quarter = half // 2
    inverse = ROPE_BASE ** (-np.arange(quarter, dtype=np.float64) * (2.0 / half))
    channel = np.arange(LANES) % head_dim
    freq = inverse[channel % quarter]
    sign = np.where(channel % half < quarter, -1.0, 1.0)
    by_row = channel < half

    def table(count, lanes):
        angles = np.arange(count, dtype=np.float64)[:, None] * freq[None, :]
        cosine = np.where(lanes[None, :], np.cos(angles), 0.0)
        sine = np.where(lanes[None, :], np.sin(angles) * sign[None, :], 0.0)
        return np.concatenate([cosine, sine], axis=1)

    pad = -n_rows % 8
    rows = np.concatenate([table(n_rows, by_row), np.zeros((pad, 2 * LANES))])
    return np.concatenate([table(GRID_W, ~by_row), rows]).astype(np.float32)


def turn(values, row_start, table_ref, head_dim):
    quarter = head_dim // 4
    rows = values.shape[0]
    lane = lax.broadcasted_iota(jnp.int32, (1, LANES), 1)
    ahead = pltpu.roll(values, LANES - quarter, 1)
    behind = pltpu.roll(values, quarter, 1)
    other = jnp.where(lane % (2 * quarter) < quarter, ahead, behind)
    columns = table_ref[0:GRID_W, :]
    out = []
    for j in range(rows // GRID_W):
        row = table_ref[pl.ds(GRID_W + row_start + j, 1), :]
        both = columns + row
        part = slice(j * GRID_W, (j + 1) * GRID_W)
        out.append(values[part] * both[:, :LANES] + other[part] * both[:, LANES:])
    return jnp.concatenate(out, axis=0)


def normed(values, gain, head_dim):
    lane = lax.broadcasted_iota(jnp.int32, (1, LANES), 1)
    gain = jnp.concatenate([gain] * (LANES // head_dim), axis=1)
    squares = values * values
    scale = jnp.zeros_like(values)
    for g in range(LANES // head_dim):
        mine = lane // head_dim == g
        mean = jnp.sum(jnp.where(mine, squares, 0.0), axis=1, keepdims=True) * (1.0 / head_dim)
        scale = jnp.where(mine, lax.rsqrt(mean + NORM_EPS), scale)
    return values * scale * gain


class Copies:
    def __init__(self, sems):
        self.sems = sems
        self.held = []

    def start(self, src, dst):
        copy = pltpu.make_async_copy(src, dst, self.sems.at[len(self.held)])
        copy.start()
        self.held.append(copy)

    def wait(self, first, last):
        for copy in self.held[first:last]:
            copy.wait()


def kv_kernel(
    head_dim, pieces, tok_hbm, wk_hbm, wv_hbm, gain_hbm, table_hbm,
    out_ref, tok_ref, both_ref, gain_ref, table_ref, sems,
):
    rows, width = tok_ref.shape
    step = width // pieces
    copies = Copies(sems)
    for i in range(pieces):
        part = pl.ds(i * step, step)
        copies.start(tok_hbm.at[:, part], tok_ref.at[:, part])
        copies.start(wk_hbm.at[:, part], both_ref.at[pl.ds(0, head_dim), part])
        copies.start(wv_hbm.at[:, part], both_ref.at[pl.ds(head_dim, head_dim), part])
    copies.start(gain_hbm, gain_ref)
    copies.start(table_hbm.at[:, pl.ds(0, 2 * LANES)], table_ref)
    raw = None
    for i in range(pieces):
        copies.wait(3 * i, 3 * i + 3)
        part = slice(i * step, (i + 1) * step)
        more = lax.dot_general(
            tok_ref[:, part], both_ref[:, part], NT, preferred_element_type=jnp.float32
        )
        raw = more if raw is None else raw + more
    raw = raw.astype(jnp.bfloat16).astype(jnp.float32)
    lane = lax.broadcasted_iota(jnp.int32, (1, LANES), 1)
    row_start = lax.axis_index("sp") * (rows // GRID_W)
    copies.wait(3 * pieces, 3 * pieces + 2)
    keys = turn(normed(raw, gain_ref[...], head_dim), row_start, table_ref, head_dim)
    out_ref[...] = jnp.where(lane < head_dim, keys, raw).astype(jnp.bfloat16)


def attend(qt, kv, head_dim, top, total, acc):
    scores = jnp.dot(kv, qt, preferred_element_type=jnp.float32)
    length, width = scores.shape
    new_top = jnp.max(scores, axis=0, keepdims=True)
    if top is not None:
        new_top = jnp.maximum(top, new_top)
    expos = jnp.exp(scores - new_top)
    part = jnp.sum(expos.reshape(length // 8, 8, width), axis=0)
    values = kv.astype(jnp.float32).T[head_dim : 2 * head_dim].astype(jnp.bfloat16)
    fresh = jnp.dot(values, expos.astype(jnp.bfloat16), preferred_element_type=jnp.float32)
    if top is None:
        return new_top, part, fresh
    shrink = jnp.exp(top - new_top)
    return new_top, total * shrink + part, acc * shrink + fresh


def attend_all(qt_ref, kv_refs, head_dim, state):
    for kv_ref in kv_refs:
        length = kv_ref.shape[0]
        step = length
        while step > 512:
            step //= 2
        if length == step:
            state = attend(qt_ref[...], kv_ref[...], head_dim, *state)
        else:

            def body(i, carry, kv_ref=kv_ref, step=step):
                at = pl.multiple_of(i * step, step)
                return attend(qt_ref[...], kv_ref[pl.ds(at, step), :], head_dim, *carry)

            state = lax.fori_loop(0, length // step, body, state)
    return state


def q_kernel(head_dim, tok_ref, wq_ref, gain_ref, table_ref, qt_ref):
    rows = tok_ref.shape[0]
    heads = wq_ref.shape[1] // head_dim
    raw = jnp.dot(tok_ref[...], wq_ref[...], preferred_element_type=jnp.float32)
    raw = raw.astype(jnp.bfloat16).astype(jnp.float32)
    row_start = lax.axis_index("sp") * (rows // GRID_W)
    per = LANES // head_dim
    columns = []
    for p in range(heads // per):
        x = raw[:, p * LANES : (p + 1) * LANES]
        y = turn(normed(x, gain_ref[...], head_dim), row_start, table_ref, head_dim)
        yt = (y * (head_dim ** -0.5)).T
        columns += [yt[g * head_dim : (g + 1) * head_dim] for g in range(per)]
    qt = jnp.concatenate(columns, axis=1)
    qt = jnp.concatenate([qt, jnp.zeros((LANES - head_dim, qt.shape[1]), jnp.float32)], axis=0)
    qt_ref[...] = qt.astype(jnp.bfloat16)


def first_kernel(head_dim, qt_ref, *refs):
    kv_refs = refs[:-3]
    top_ref, total_ref, acc_ref = refs[-3:]
    state = attend_all(qt_ref, kv_refs, head_dim, (None, None, None))
    top_ref[...], total_ref[...], acc_ref[...] = state


def block_kernel(head_dim, qt_ref, *refs):
    kv_refs = refs[:-6]
    top_in, total_in, acc_in, top_ref, total_ref, acc_ref = refs[-6:]
    state = attend_all(qt_ref, kv_refs, head_dim, (top_in[...], total_in[...], acc_in[...]))
    top_ref[...], total_ref[...], acc_ref[...] = state


def finish_kernel(head_dim, qt_ref, *refs):
    kv_refs = refs[:-5]
    top_in, total_in, acc_in, att_ref, log_ref = refs[-5:]
    state = attend_all(qt_ref, kv_refs, head_dim, (top_in[...], total_in[...], acc_in[...]))
    top, total, acc = state
    summed = jnp.sum(total, axis=0, keepdims=True)
    log = top + jnp.log(summed)
    out = acc / summed
    rows = att_ref.shape[0]
    heads = log_ref.shape[0]
    per = LANES // head_dim
    for h in range(heads):
        log_ref[h : h + 1, :] = log[:, h * rows : (h + 1) * rows]
    for p in range(heads // per):
        pair = [out[:, h * rows : (h + 1) * rows] for h in range(p * per, (p + 1) * per)]
        att = jnp.concatenate(pair, axis=0).T
        att_ref[:, p * LANES : (p + 1) * LANES] = att.astype(jnp.bfloat16)


def call(kernel, out_shape, flops, in_specs, limit=LIMIT, **more):
    return pl.pallas_call(
        kernel,
        out_shape=out_shape,
        in_specs=in_specs,
        out_specs=jax.tree.map(lambda _: VMEM, out_shape),
        cost_estimate=pl.CostEstimate(flops=flops, bytes_accessed=flops // 256, transcendentals=0),
        compiler_params=pltpu.CompilerParams(vmem_limit_bytes=limit),
        **more,
    )


def xor(n, bit):
    return [(i, i ^ bit) for i in range(n)]


def shards(n_sp, n_tp, tokens, w_query, w_key, w_value, w_output, query_gain, key_gain):
    head_dim = query_gain.shape[0]
    rows, width = tokens.shape
    heads = w_query.shape[1] // head_dim
    table = rope_tables(n_sp * rows // GRID_W, head_dim)
    wide = jnp.asarray(np.pad(table, ((0, 0), (0, 7 * table.shape[1]))))
    table = jnp.asarray(table)
    f32 = functools.partial(jax.ShapeDtypeStruct, dtype=jnp.float32)
    bf16 = functools.partial(jax.ShapeDtypeStruct, dtype=jnp.bfloat16)
    pieces = 4

    scratch = [pltpu.VMEM((1, head_dim), jnp.float32), pltpu.VMEM((table.shape[0], 2 * LANES), jnp.float32)]
    kv = call(
        functools.partial(kv_kernel, head_dim, pieces),
        bf16((rows, LANES)),
        2 * rows * width * LANES,
        [HBM] * 5,
        KV_LIMIT,
        scratch_shapes=[
            pltpu.VMEM(tokens.shape, jnp.bfloat16),
            pltpu.VMEM((LANES, width), jnp.bfloat16),
            *scratch,
            pltpu.SemaphoreType.DMA((3 * pieces + 2,)),
        ],
    )(tokens, w_key.T, w_value.T, key_gain[None, :], wide)

    size = heads * rows
    state_shape = [f32((1, size)), f32((8, size)), f32((head_dim, size))]

    def work(kvs):
        return sum(4 * size * x.shape[0] * LANES for x in kvs)

    qt = call(
        functools.partial(q_kernel, head_dim),
        bf16((LANES, size)),
        2 * rows * width * heads * head_dim,
        [VMEM] * 4,
    )(tokens, w_query, query_gain[None, :], table)

    def first(qt, *kvs):
        return call(
            functools.partial(first_kernel, head_dim),
            state_shape,
            work(kvs),
            [VMEM] * (1 + len(kvs)),
        )(qt, *kvs)

    def blocks(qt, state, *kvs):
        return call(
            functools.partial(block_kernel, head_dim),
            state_shape,
            work(kvs),
            [VMEM] * (4 + len(kvs)),
            input_output_aliases={1 + len(kvs) + i: i for i in range(3)},
        )(qt, *kvs, *state)

    def finish(qt, state, *kvs):
        return call(
            functools.partial(finish_kernel, head_dim),
            [bf16((rows, heads * head_dim)), f32((heads, rows))],
            work(kvs),
            [VMEM] * (4 + len(kvs)),
        )(qt, *kvs, *state)

    send = functools.partial(lax.ppermute, axis_name="sp")
    if n_sp == 8:
        near = send(kv, perm=xor(n_sp, 1))
        far = send(kv, perm=xor(n_sp, 6))
        pair = jnp.concatenate([kv, near], axis=0)
        middle = send(pair, perm=xor(n_sp, 4))
        beside = send(pair, perm=xor(n_sp, 2))
        far, qt = lax.optimization_barrier((far, qt))
        relayed = send(far, perm=xor(n_sp, 1))
        state = first(qt, pair)
        state = blocks(qt, state, beside)
        attended, log_sums = finish(qt, state, far, middle, relayed)
    else:
        held = kv
        state = None
        stride = 1
        pending = [kv]
        while stride < n_sp:
            radix = 2 if stride == 1 else min(4, n_sp // stride)
            got = [send(held, perm=xor(n_sp, d * stride)) for d in range(1, radix)]
            if state is None:
                state = first(qt, *pending)
            else:
                state = blocks(qt, state, *pending)
            pending = got
            stride *= radix
            if stride < n_sp:
                held = jnp.concatenate([held] + got, axis=0)
        attended, log_sums = finish(qt, state, *pending)

    own = rows // n_tp
    me = lax.axis_index("tp")

    def partial_out(block):
        part = lax.dynamic_slice_in_dim(attended, block * own, own, 0)
        return jnp.dot(part, w_output, preferred_element_type=jnp.float32)

    parts = {d: partial_out(me ^ d) for d in range(n_tp)}
    b = 1
    while b < n_tp:
        left = [d for d in parts if not d & b]
        sent = jnp.concatenate([parts[d ^ b].astype(jnp.bfloat16) for d in left], axis=0)
        got = lax.ppermute(sent, "tp", xor(n_tp, b)).astype(jnp.float32)
        parts = {d: parts[d] + got[i * own : (i + 1) * own] for i, d in enumerate(left)}
        b *= 2
    return parts[0].astype(jnp.bfloat16), log_sums


def solution(mesh):
    placed = (P("sp", None), P(None, "tp"), P(None, "tp"), P(None, "tp"), P("tp", None), P(), P())
    return jax.shard_map(
        functools.partial(shards, mesh.shape["sp"], mesh.shape["tp"]),
        mesh=mesh,
        in_specs=placed,
        out_specs=(P(("sp", "tp"), None), P("tp", "sp")),
        check_vma=False,
    )
```

```python
import functools

import jax
import jax.numpy as jnp
import numpy as np
from jax import lax
from jax.experimental import pallas as pl
from jax.experimental.pallas import tpu as pltpu
from jax.sharding import PartitionSpec as P


GRID_W = 64
ROPE_BASE = 10000.0
NORM_EPS = 1e-06
LANES = 128
LIMIT = 12 << 20
KV_LIMIT = 56480000


VMEM = pl.BlockSpec(memory_space=pltpu.VMEM)
HBM = pl.BlockSpec(memory_space=pltpu.HBM)
NT = (((1,), (1,)), ((), ()))


def rope_tables(n_rows, head_dim):
    half = head_dim // 2
    quarter = half // 2
    inverse = ROPE_BASE ** (-np.arange(quarter, dtype=np.float64) * (2.0 / half))
    channel = np.arange(LANES) % head_dim
    freq = inverse[channel % quarter]
    sign = np.where(channel % half < quarter, -1.0, 1.0)
    by_row = channel < half

    def table(count, lanes):
        angles = np.arange(count, dtype=np.float64)[:, None] * freq[None, :]
        cosine = np.where(lanes[None, :], np.cos(angles), 0.0)
        sine = np.where(lanes[None, :], np.sin(angles) * sign[None, :], 0.0)
        return np.concatenate([cosine, sine], axis=1)

    pad = -n_rows % 8
    rows = np.concatenate([table(n_rows, by_row), np.zeros((pad, 2 * LANES))])
    return np.concatenate([table(GRID_W, ~by_row), rows]).astype(np.float32)


def turn(values, row_start, table_ref, head_dim):
    quarter = head_dim // 4
    rows = values.shape[0]
    lane = lax.broadcasted_iota(jnp.int32, (1, LANES), 1)
    ahead = pltpu.roll(values, LANES - quarter, 1)
    behind = pltpu.roll(values, quarter, 1)
    other = jnp.where(lane % (2 * quarter) < quarter, ahead, behind)
    columns = table_ref[0:GRID_W, :]
    out = []
    for j in range(rows // GRID_W):
        row = table_ref[pl.ds(GRID_W + row_start + j, 1), :]
        both = columns + row
        part = slice(j * GRID_W, (j + 1) * GRID_W)
        out.append(values[part] * both[:, :LANES] + other[part] * both[:, LANES:])
    return jnp.concatenate(out, axis=0)


def normed(values, gain, head_dim):
    lane = lax.broadcasted_iota(jnp.int32, (1, LANES), 1)
    gain = jnp.concatenate([gain] * (LANES // head_dim), axis=1)
    squares = values * values
    scale = jnp.zeros_like(values)
    for g in range(LANES // head_dim):
        mine = lane // head_dim == g
        mean = jnp.sum(jnp.where(mine, squares, 0.0), axis=1, keepdims=True) * (1.0 / head_dim)
        scale = jnp.where(mine, lax.rsqrt(mean + NORM_EPS), scale)
    return values * scale * gain


class Copies:
    def __init__(self, sems):
        self.sems = sems
        self.held = []

    def start(self, src, dst):
        copy = pltpu.make_async_copy(src, dst, self.sems.at[len(self.held)])
        copy.start()
        self.held.append(copy)

    def wait(self, first, last):
        for copy in self.held[first:last]:
            copy.wait()


def kv_kernel(
    head_dim, pieces, tok_hbm, wk_hbm, wv_hbm, gain_hbm, table_hbm,
    out_ref, tok_ref, both_ref, gain_ref, table_ref, sems,
):
    rows, width = tok_ref.shape
    step = width // pieces
    copies = Copies(sems)
    for i in range(pieces):
        part = pl.ds(i * step, step)
        copies.start(tok_hbm.at[:, part], tok_ref.at[:, part])
        copies.start(wk_hbm.at[:, part], both_ref.at[pl.ds(0, head_dim), part])
        copies.start(wv_hbm.at[:, part], both_ref.at[pl.ds(head_dim, head_dim), part])
    copies.start(gain_hbm, gain_ref)
    copies.start(table_hbm.at[:, pl.ds(0, 2 * LANES)], table_ref)
    raw = None
    for i in range(pieces):
        copies.wait(3 * i, 3 * i + 3)
        part = slice(i * step, (i + 1) * step)
        more = lax.dot_general(
            tok_ref[:, part], both_ref[:, part], NT, preferred_element_type=jnp.float32
        )
        raw = more if raw is None else raw + more
    raw = raw.astype(jnp.bfloat16).astype(jnp.float32)
    lane = lax.broadcasted_iota(jnp.int32, (1, LANES), 1)
    row_start = lax.axis_index("sp") * (rows // GRID_W)
    copies.wait(3 * pieces, 3 * pieces + 2)
    keys = turn(normed(raw, gain_ref[...], head_dim), row_start, table_ref, head_dim)
    out_ref[...] = jnp.where(lane < head_dim, keys, raw).astype(jnp.bfloat16)


def attend(qt, kv, head_dim, top, total, acc):
    scores = jnp.dot(kv, qt, preferred_element_type=jnp.float32)
    length, width = scores.shape
    new_top = jnp.max(scores, axis=0, keepdims=True)
    if top is not None:
        new_top = jnp.maximum(top, new_top)
    expos = jnp.exp(scores - new_top)
    part = jnp.sum(expos.reshape(length // 8, 8, width), axis=0)
    values = kv.astype(jnp.float32).T[head_dim : 2 * head_dim].astype(jnp.bfloat16)
    fresh = jnp.dot(values, expos.astype(jnp.bfloat16), preferred_element_type=jnp.float32)
    if top is None:
        return new_top, part, fresh
    shrink = jnp.exp(top - new_top)
    return new_top, total * shrink + part, acc * shrink + fresh


def attend_all(qt_ref, kv_refs, head_dim, state):
    for kv_ref in kv_refs:
        length = kv_ref.shape[0]
        step = length
        while step > 512:
            step //= 2
        if length == step:
            state = attend(qt_ref[...], kv_ref[...], head_dim, *state)
        else:

            def body(i, carry, kv_ref=kv_ref, step=step):
                at = pl.multiple_of(i * step, step)
                return attend(qt_ref[...], kv_ref[pl.ds(at, step), :], head_dim, *carry)

            state = lax.fori_loop(0, length // step, body, state)
    return state


def q_kernel(head_dim, tok_ref, wq_ref, gain_ref, table_ref, qt_ref):
    rows = tok_ref.shape[0]
    heads = wq_ref.shape[1] // head_dim
    raw = jnp.dot(tok_ref[...], wq_ref[...], preferred_element_type=jnp.float32)
    raw = raw.astype(jnp.bfloat16).astype(jnp.float32)
    row_start = lax.axis_index("sp") * (rows // GRID_W)
    per = LANES // head_dim
    columns = []
    for p in range(heads // per):
        x = raw[:, p * LANES : (p + 1) * LANES]
        y = turn(normed(x, gain_ref[...], head_dim), row_start, table_ref, head_dim)
        yt = (y * (head_dim ** -0.5)).T
        columns += [yt[g * head_dim : (g + 1) * head_dim] for g in range(per)]
    qt = jnp.concatenate(columns, axis=1)
    qt = jnp.concatenate([qt, jnp.zeros((LANES - head_dim, qt.shape[1]), jnp.float32)], axis=0)
    qt_ref[...] = qt.astype(jnp.bfloat16)


def first_kernel(head_dim, qt_ref, *refs):
    kv_refs = refs[:-3]
    top_ref, total_ref, acc_ref = refs[-3:]
    state = attend_all(qt_ref, kv_refs, head_dim, (None, None, None))
    top_ref[...], total_ref[...], acc_ref[...] = state


def block_kernel(head_dim, qt_ref, *refs):
    kv_refs = refs[:-6]
    top_in, total_in, acc_in, top_ref, total_ref, acc_ref = refs[-6:]
    state = attend_all(qt_ref, kv_refs, head_dim, (top_in[...], total_in[...], acc_in[...]))
    top_ref[...], total_ref[...], acc_ref[...] = state


def finish_kernel(head_dim, qt_ref, *refs):
    kv_refs = refs[:-8]
    top_in, total_in, acc_in, wo_ref, att_ref, top_ref, sum_ref, sent_ref = refs[-8:]
    state = attend_all(qt_ref, kv_refs, head_dim, (top_in[...], total_in[...], acc_in[...]))
    top, total, acc = state
    summed = jnp.sum(total, axis=0, keepdims=True)
    out = acc * (1.0 / summed)
    rows = att_ref.shape[0]
    heads = top_ref.shape[0]
    per = LANES // head_dim
    for p in range(heads // per):
        pair = [out[:, h * rows : (h + 1) * rows] for h in range(p * per, (p + 1) * per)]
        att = jnp.concatenate(pair, axis=0).T
        att_ref[:, p * LANES : (p + 1) * LANES] = att.astype(jnp.bfloat16)
    own = sent_ref.shape[0]
    sent_ref[...] = product(att_ref, wo_ref, rows // own - 1, own).astype(jnp.bfloat16)
    for h in range(heads):
        top_ref[h : h + 1, :] = top[:, h * rows : (h + 1) * rows]
        sum_ref[h : h + 1, :] = summed[:, h * rows : (h + 1) * rows]


def product(att_ref, wo_ref, d, own):
    at = pl.multiple_of((lax.axis_index("tp") ^ d) * own, own)
    return jnp.dot(att_ref[pl.ds(at, own), :], wo_ref[...], preferred_element_type=jnp.float32)


def rest_kernel(att_ref, wo_ref, *out_refs):
    for d, out_ref in enumerate(out_refs):
        out = product(att_ref, wo_ref, d, out_ref.shape[0])
        out_ref[...] = out.astype(out_ref.dtype)


def call(kernel, out_shape, flops, in_specs, limit=LIMIT, **more):
    return pl.pallas_call(
        kernel,
        out_shape=out_shape,
        in_specs=in_specs,
        out_specs=jax.tree.map(lambda _: VMEM, out_shape),
        cost_estimate=pl.CostEstimate(flops=flops, bytes_accessed=flops // 256, transcendentals=0),
        compiler_params=pltpu.CompilerParams(vmem_limit_bytes=limit),
        **more,
    )


def xor(n, bit):
    return [(i, i ^ bit) for i in range(n)]


def shards(n_sp, n_tp, tokens, w_query, w_key, w_value, w_output, query_gain, key_gain):
    head_dim = query_gain.shape[0]
    rows, width = tokens.shape
    heads = w_query.shape[1] // head_dim
    table = rope_tables(n_sp * rows // GRID_W, head_dim)
    wide = jnp.asarray(np.pad(table, ((0, 0), (0, 7 * table.shape[1]))))
    table = jnp.asarray(table)
    f32 = functools.partial(jax.ShapeDtypeStruct, dtype=jnp.float32)
    bf16 = functools.partial(jax.ShapeDtypeStruct, dtype=jnp.bfloat16)
    pieces = 1

    scratch = [pltpu.VMEM((1, head_dim), jnp.float32), pltpu.VMEM((table.shape[0], 2 * LANES), jnp.float32)]
    kv = call(
        functools.partial(kv_kernel, head_dim, pieces),
        bf16((rows, LANES)),
        2 * rows * width * LANES,
        [HBM] * 5,
        KV_LIMIT,
        scratch_shapes=[
            pltpu.VMEM(tokens.shape, jnp.bfloat16),
            pltpu.VMEM((LANES, width), jnp.bfloat16),
            *scratch,
            pltpu.SemaphoreType.DMA((3 * pieces + 2,)),
        ],
    )(tokens, w_key.T, w_value.T, key_gain[None, :], wide)

    kv, tokens, w_query, w_output = lax.optimization_barrier((kv, tokens, w_query, w_output))
    size = heads * rows
    state_shape = [f32((1, size)), f32((8, size)), f32((head_dim, size))]

    def work(kvs):
        return sum(4 * size * x.shape[0] * LANES for x in kvs)

    qt = call(
        functools.partial(q_kernel, head_dim),
        bf16((LANES, size)),
        2 * rows * width * heads * head_dim,
        [VMEM] * 4,
    )(tokens, w_query, query_gain[None, :], table)

    def first(qt, *kvs):
        return call(
            functools.partial(first_kernel, head_dim),
            state_shape,
            work(kvs),
            [VMEM] * (1 + len(kvs)),
        )(qt, *kvs)

    def blocks(qt, state, *kvs):
        return call(
            functools.partial(block_kernel, head_dim),
            state_shape,
            work(kvs),
            [VMEM] * (4 + len(kvs)),
            input_output_aliases={1 + len(kvs) + i: i for i in range(3)},
        )(qt, *kvs, *state)

    own = rows // n_tp

    def finish(qt, state, *kvs):
        return call(
            functools.partial(finish_kernel, head_dim),
            [
                bf16((rows, heads * head_dim)),
                f32((heads, rows)),
                f32((heads, rows)),
                bf16((own, w_output.shape[1])),
            ],
            work(kvs),
            [VMEM] * (5 + len(kvs)),
        )(qt, *kvs, *state, w_output)

    send = functools.partial(lax.ppermute, axis_name="sp")
    if n_sp == 8:
        near = send(kv, perm=xor(n_sp, 1))
        far = send(kv, perm=xor(n_sp, 6))
        pair = jnp.concatenate([kv, near], axis=0)
        middle = send(pair, perm=xor(n_sp, 4))
        beside = send(pair, perm=xor(n_sp, 2))
        relayed = send(far, perm=xor(n_sp, 1))
        state = first(qt, pair)
        state = blocks(qt, state, beside, far)
        state = blocks(qt, state, relayed)
        attended, top, summed, sent = finish(qt, state, middle)
    else:
        held = kv
        state = None
        stride = 1
        pending = [kv]
        while stride < n_sp:
            radix = 2 if stride == 1 else min(4, n_sp // stride)
            got = [send(held, perm=xor(n_sp, d * stride)) for d in range(1, radix)]
            if state is None:
                state = first(qt, *pending)
            else:
                state = blocks(qt, state, *pending)
            pending = got
            stride *= radix
            if stride < n_sp:
                held = jnp.concatenate([held] + got, axis=0)
        attended, top, summed, sent = finish(qt, state, *pending)

    parts = call(
        rest_kernel,
        [(bf16 if d % 2 else f32)(sent.shape) for d in range(n_tp - 1)],
        2 * rows * w_output.size // n_tp,
        [VMEM] * 2,
    )(attended, w_output)
    parts = [*parts, sent]
    bit = 1
    while bit < n_tp:
        for d in reversed(range(0, n_tp, 2 * bit)):
            got = lax.ppermute(parts[d + bit].astype(jnp.bfloat16), "tp", xor(n_tp, bit))
            parts[d] = parts[d] + got.astype(jnp.float32)
        bit *= 2
    return parts[0].astype(jnp.bfloat16), top + jnp.log(summed)


def solution(mesh):
    placed = (P("sp", None), P(None, "tp"), P(None, "tp"), P(None, "tp"), P("tp", None), P(), P())
    return jax.shard_map(
        functools.partial(shards, mesh.shape["sp"], mesh.shape["tp"]),
        mesh=mesh,
        in_specs=placed,
        out_specs=(P(("sp", "tp"), None), P("tp", "sp")),
        check_vma=False,
    )
```

```python
import functools

import jax
import jax.numpy as jnp
import numpy as np
from jax import lax
from jax.experimental import pallas as pl
from jax.experimental.pallas import tpu as pltpu
from jax.sharding import PartitionSpec as P


GRID_W = 64
ROPE_BASE = 10000.0
NORM_EPS = 1e-06
LANES = 128
LIMIT = 12 << 20
SPAN = 768
KV_LIMIT = 56480000


VMEM = pl.BlockSpec(memory_space=pltpu.VMEM)
HBM = pl.BlockSpec(memory_space=pltpu.HBM)
NT = (((1,), (1,)), ((), ()))


def rope_tables(n_rows, head_dim):
    half = head_dim // 2
    quarter = half // 2
    inverse = ROPE_BASE ** (-np.arange(quarter, dtype=np.float64) * (2.0 / half))
    channel = np.arange(LANES) % head_dim
    freq = inverse[channel % quarter]
    sign = np.where(channel % half < quarter, -1.0, 1.0)
    by_row = channel < half

    def table(count, lanes):
        angles = np.arange(count, dtype=np.float64)[:, None] * freq[None, :]
        cosine = np.where(lanes[None, :], np.cos(angles), 0.0)
        sine = np.where(lanes[None, :], np.sin(angles) * sign[None, :], 0.0)
        return np.concatenate([cosine, sine], axis=1)

    pad = -n_rows % 8
    rows = np.concatenate([table(n_rows, by_row), np.zeros((pad, 2 * LANES))])
    return np.concatenate([table(GRID_W, ~by_row), rows]).astype(np.float32)


def turn(values, row_start, table_ref, head_dim):
    quarter = head_dim // 4
    rows = values.shape[0]
    lane = lax.broadcasted_iota(jnp.int32, (1, LANES), 1)
    ahead = pltpu.roll(values, LANES - quarter, 1)
    behind = pltpu.roll(values, quarter, 1)
    other = jnp.where(lane % (2 * quarter) < quarter, ahead, behind)
    columns = table_ref[0:GRID_W, :]
    out = []
    for j in range(rows // GRID_W):
        row = table_ref[pl.ds(GRID_W + row_start + j, 1), :]
        both = columns + row
        part = slice(j * GRID_W, (j + 1) * GRID_W)
        out.append(values[part] * both[:, :LANES] + other[part] * both[:, LANES:])
    return jnp.concatenate(out, axis=0)


def normed(values, gain, head_dim):
    lane = lax.broadcasted_iota(jnp.int32, (1, LANES), 1)
    gain = jnp.concatenate([gain] * (LANES // head_dim), axis=1)
    squares = values * values
    scale = jnp.zeros_like(values)
    for g in range(LANES // head_dim):
        mine = lane // head_dim == g
        mean = jnp.sum(jnp.where(mine, squares, 0.0), axis=1, keepdims=True) * (1.0 / head_dim)
        scale = jnp.where(mine, lax.rsqrt(mean + NORM_EPS), scale)
    return values * scale * gain


class Copies:
    def __init__(self, sems):
        self.sems = sems
        self.held = []

    def start(self, src, dst):
        copy = pltpu.make_async_copy(src, dst, self.sems.at[len(self.held)])
        copy.start()
        self.held.append(copy)

    def wait(self, first, last):
        for copy in self.held[first:last]:
            copy.wait()


def kv_kernel(
    head_dim, pieces, tok_hbm, wk_hbm, wv_hbm, gain_hbm, table_hbm,
    out_ref, tok_ref, both_ref, gain_ref, table_ref, sems,
):
    rows, width = tok_ref.shape
    step = width // pieces
    copies = Copies(sems)
    for i in range(pieces):
        part = pl.ds(i * step, step)
        copies.start(tok_hbm.at[:, part], tok_ref.at[:, part])
        copies.start(wk_hbm.at[:, part], both_ref.at[pl.ds(0, head_dim), part])
        copies.start(wv_hbm.at[:, part], both_ref.at[pl.ds(head_dim, head_dim), part])
    copies.start(gain_hbm, gain_ref)
    copies.start(table_hbm.at[:, pl.ds(0, 2 * LANES)], table_ref)
    raw = None
    for i in range(pieces):
        copies.wait(3 * i, 3 * i + 3)
        part = slice(i * step, (i + 1) * step)
        more = lax.dot_general(
            tok_ref[:, part], both_ref[:, part], NT, preferred_element_type=jnp.float32
        )
        raw = more if raw is None else raw + more
    raw = raw.astype(jnp.bfloat16).astype(jnp.float32)
    lane = lax.broadcasted_iota(jnp.int32, (1, LANES), 1)
    row_start = lax.axis_index("sp") * (rows // GRID_W)
    copies.wait(3 * pieces, 3 * pieces + 2)
    keys = turn(normed(raw, gain_ref[...], head_dim), row_start, table_ref, head_dim)
    out_ref[...] = jnp.where(lane < head_dim, keys, raw).astype(jnp.bfloat16)


def attend(qt, kvs, head_dim, top, total, acc, score_ref, weight_ref):
    width = qt.shape[1]
    count = 0
    eight = None
    values = []
    for kv in kvs:
        scores = jnp.dot(kv, qt, preferred_element_type=jnp.float32)
        score_ref[count : count + kv.shape[0], :] = scores
        for i in range(0, kv.shape[0], 8):
            most = score_ref[count + i : count + i + 8, :]
            eight = most if eight is None else jnp.maximum(eight, most)
        values.append(kv.astype(jnp.float32).T[head_dim : 2 * head_dim].astype(jnp.bfloat16))
        count += kv.shape[0]
    new_top = jnp.max(eight, axis=0, keepdims=True)
    if top is not None:
        new_top = jnp.maximum(top, new_top)
    part = jnp.zeros((8, width), jnp.float32)
    for at in range(0, count, 16):
        expos = jnp.exp(score_ref[at : at + 16, :] - new_top)
        weight_ref[at : at + 16, :] = expos.astype(jnp.bfloat16)
        part = part + (expos[:8] + expos[8:])
    values = jnp.concatenate(values, axis=1)
    fresh = jnp.dot(values, weight_ref[0:count, :], preferred_element_type=jnp.float32)
    if top is None:
        return new_top, part, fresh
    shrink = jnp.exp(top - new_top)
    return new_top, total * shrink + part, acc * shrink + fresh


def attend_all(qt_ref, kv_refs, head_dim, state, score_ref, weight_ref):
    spare = head_dim, *state, score_ref, weight_ref
    if sum(kv_ref.shape[0] for kv_ref in kv_refs) <= SPAN:
        return attend(qt_ref[...], [kv_ref[...] for kv_ref in kv_refs], *spare)
    for kv_ref in kv_refs:
        length = kv_ref.shape[0]
        step = length
        while step > SPAN:
            step //= 2
        if length == step:
            state = attend(qt_ref[...], [kv_ref[...]], head_dim, *state, score_ref, weight_ref)
        else:

            def body(i, carry, kv_ref=kv_ref, step=step):
                at = pl.multiple_of(i * step, step)
                kvs = [kv_ref[pl.ds(at, step), :]]
                return attend(qt_ref[...], kvs, head_dim, *carry, score_ref, weight_ref)

            state = lax.fori_loop(0, length // step, body, state)
    return state


def q_kernel(head_dim, tok_ref, wq_ref, gain_ref, table_ref, qt_ref):
    rows = tok_ref.shape[0]
    heads = wq_ref.shape[1] // head_dim
    raw = jnp.dot(tok_ref[...], wq_ref[...], preferred_element_type=jnp.float32)
    raw = raw.astype(jnp.bfloat16).astype(jnp.float32)
    row_start = lax.axis_index("sp") * (rows // GRID_W)
    per = LANES // head_dim
    columns = []
    for p in range(heads // per):
        x = raw[:, p * LANES : (p + 1) * LANES]
        y = turn(normed(x, gain_ref[...], head_dim), row_start, table_ref, head_dim)
        yt = (y * (head_dim ** -0.5)).T
        columns += [yt[g * head_dim : (g + 1) * head_dim] for g in range(per)]
    qt = jnp.concatenate(columns, axis=1)
    qt = jnp.concatenate([qt, jnp.zeros((LANES - head_dim, qt.shape[1]), jnp.float32)], axis=0)
    qt_ref[...] = qt.astype(jnp.bfloat16)


def first_kernel(head_dim, qt_ref, *refs):
    kv_refs = refs[:-5]
    top_ref, total_ref, acc_ref, *spare = refs[-5:]
    state = attend_all(qt_ref, kv_refs, head_dim, (None, None, None), *spare)
    top_ref[...], total_ref[...], acc_ref[...] = state


def block_kernel(head_dim, qt_ref, *refs):
    kv_refs = refs[:-8]
    top_in, total_in, acc_in, top_ref, total_ref, acc_ref, *spare = refs[-8:]
    state = attend_all(qt_ref, kv_refs, head_dim, (top_in[...], total_in[...], acc_in[...]), *spare)
    top_ref[...], total_ref[...], acc_ref[...] = state


def finish_kernel(head_dim, qt_ref, *refs):
    kv_refs = refs[:-10]
    top_in, total_in, acc_in, wo_ref, att_ref, top_ref, sum_ref, sent_ref, *spare = refs[-10:]
    state = attend_all(qt_ref, kv_refs, head_dim, (top_in[...], total_in[...], acc_in[...]), *spare)
    top, total, acc = state
    summed = jnp.sum(total, axis=0, keepdims=True)
    out = acc * (1.0 / summed)
    rows = att_ref.shape[0]
    heads = top_ref.shape[0]
    per = LANES // head_dim
    for p in range(heads // per):
        pair = [out[:, h * rows : (h + 1) * rows] for h in range(p * per, (p + 1) * per)]
        att = jnp.concatenate(pair, axis=0).T
        att_ref[:, p * LANES : (p + 1) * LANES] = att.astype(jnp.bfloat16)
    own = sent_ref.shape[0]
    sent_ref[...] = product(att_ref, wo_ref, rows // own - 1, own).astype(jnp.bfloat16)
    for h in range(heads):
        top_ref[h : h + 1, :] = top[:, h * rows : (h + 1) * rows]
        sum_ref[h : h + 1, :] = summed[:, h * rows : (h + 1) * rows]


def product(att_ref, wo_ref, d, own):
    at = pl.multiple_of((lax.axis_index("tp") ^ d) * own, own)
    return jnp.dot(att_ref[pl.ds(at, own), :], wo_ref[...], preferred_element_type=jnp.float32)


def rest_kernel(att_ref, wo_ref, *out_refs):
    for d, out_ref in enumerate(out_refs):
        out = product(att_ref, wo_ref, d, out_ref.shape[0])
        out_ref[...] = out.astype(out_ref.dtype)


def call(kernel, out_shape, flops, in_specs, limit=LIMIT, **more):
    return pl.pallas_call(
        kernel,
        out_shape=out_shape,
        in_specs=in_specs,
        out_specs=jax.tree.map(lambda _: VMEM, out_shape),
        cost_estimate=pl.CostEstimate(flops=flops, bytes_accessed=flops // 256, transcendentals=0),
        compiler_params=pltpu.CompilerParams(vmem_limit_bytes=limit),
        **more,
    )


def xor(n, bit):
    return [(i, i ^ bit) for i in range(n)]


def shards(n_sp, n_tp, tokens, w_query, w_key, w_value, w_output, query_gain, key_gain):
    head_dim = query_gain.shape[0]
    rows, width = tokens.shape
    heads = w_query.shape[1] // head_dim
    table = rope_tables(n_sp * rows // GRID_W, head_dim)
    wide = jnp.asarray(np.pad(table, ((0, 0), (0, 7 * table.shape[1]))))
    table = jnp.asarray(table)
    f32 = functools.partial(jax.ShapeDtypeStruct, dtype=jnp.float32)
    bf16 = functools.partial(jax.ShapeDtypeStruct, dtype=jnp.bfloat16)
    pieces = 1

    scratch = [pltpu.VMEM((1, head_dim), jnp.float32), pltpu.VMEM((table.shape[0], 2 * LANES), jnp.float32)]
    kv = call(
        functools.partial(kv_kernel, head_dim, pieces),
        bf16((rows, LANES)),
        2 * rows * width * LANES,
        [HBM] * 5,
        KV_LIMIT,
        scratch_shapes=[
            pltpu.VMEM(tokens.shape, jnp.bfloat16),
            pltpu.VMEM((LANES, width), jnp.bfloat16),
            *scratch,
            pltpu.SemaphoreType.DMA((3 * pieces + 2,)),
        ],
    )(tokens, w_key.T, w_value.T, key_gain[None, :], wide)

    kv, tokens, w_query, w_output = lax.optimization_barrier((kv, tokens, w_query, w_output))
    size = heads * rows
    state_shape = [f32((1, size)), f32((8, size)), f32((head_dim, size))]

    def spare(kvs):
        count = min(SPAN, sum(x.shape[0] for x in kvs))
        return [pltpu.VMEM((count, size), jnp.float32), pltpu.VMEM((count, size), jnp.bfloat16)]

    def work(kvs):
        return sum(4 * size * x.shape[0] * LANES for x in kvs)

    qt = call(
        functools.partial(q_kernel, head_dim),
        bf16((LANES, size)),
        2 * rows * width * heads * head_dim,
        [VMEM] * 4,
    )(tokens, w_query, query_gain[None, :], table)

    def first(qt, *kvs):
        return call(
            functools.partial(first_kernel, head_dim),
            state_shape,
            work(kvs),
            [VMEM] * (1 + len(kvs)),
            scratch_shapes=spare(kvs),
        )(qt, *kvs)

    def blocks(qt, state, *kvs):
        return call(
            functools.partial(block_kernel, head_dim),
            state_shape,
            work(kvs),
            [VMEM] * (4 + len(kvs)),
            scratch_shapes=spare(kvs),
            input_output_aliases={1 + len(kvs) + i: i for i in range(3)},
        )(qt, *kvs, *state)

    own = rows // n_tp

    def finish(qt, state, *kvs):
        return call(
            functools.partial(finish_kernel, head_dim),
            [
                bf16((rows, heads * head_dim)),
                f32((heads, rows)),
                f32((heads, rows)),
                bf16((own, w_output.shape[1])),
            ],
            work(kvs),
            [VMEM] * (5 + len(kvs)),
            scratch_shapes=spare(kvs),
        )(qt, *kvs, *state, w_output)

    send = functools.partial(lax.ppermute, axis_name="sp")
    if n_sp == 8:
        near = send(kv, perm=xor(n_sp, 1))
        far = send(kv, perm=xor(n_sp, 4))
        pair = jnp.concatenate([kv, near], axis=0)
        middle = send(pair, perm=xor(n_sp, 6))
        beside = send(pair, perm=xor(n_sp, 2))
        relayed = send(far, perm=xor(n_sp, 1))
        state = first(qt, pair)
        state = blocks(qt, state, beside, far)
        attended, top, summed, sent = finish(qt, state, relayed, middle)
    else:
        held = kv
        state = None
        stride = 1
        pending = [kv]
        while stride < n_sp:
            radix = 2 if stride == 1 else min(4, n_sp // stride)
            got = [send(held, perm=xor(n_sp, d * stride)) for d in range(1, radix)]
            if state is None:
                state = first(qt, *pending)
            else:
                state = blocks(qt, state, *pending)
            pending = got
            stride *= radix
            if stride < n_sp:
                held = jnp.concatenate([held] + got, axis=0)
        attended, top, summed, sent = finish(qt, state, *pending)

    parts = call(
        rest_kernel,
        [(bf16 if d % 2 else f32)(sent.shape) for d in range(n_tp - 1)],
        2 * rows * w_output.size // n_tp,
        [VMEM] * 2,
    )(attended, w_output)
    parts = [*parts, sent]
    bit = 1
    while bit < n_tp:
        for d in reversed(range(0, n_tp, 2 * bit)):
            got = lax.ppermute(parts[d + bit].astype(jnp.bfloat16), "tp", xor(n_tp, bit))
            parts[d] = parts[d] + got.astype(jnp.float32)
        bit *= 2
    return parts[0].astype(jnp.bfloat16), top + jnp.log(summed)


def solution(mesh):
    placed = (P("sp", None), P(None, "tp"), P(None, "tp"), P(None, "tp"), P("tp", None), P(), P())
    return jax.shard_map(
        functools.partial(shards, mesh.shape["sp"], mesh.shape["tp"]),
        mesh=mesh,
        in_specs=placed,
        out_specs=(P(("sp", "tp"), None), P("tp", "sp")),
        check_vma=False,
    )
```

```python
import functools

import jax
import jax.numpy as jnp
import numpy as np
from jax import lax
from jax.experimental import pallas as pl
from jax.experimental.pallas import tpu as pltpu
from jax.sharding import PartitionSpec as P


GRID_W = 64
ROPE_BASE = 10000.0
NORM_EPS = 1e-06
LANES = 128
LIMIT = 12 << 20
SPAN = 768
KV_LIMIT = 56480000


VMEM = pl.BlockSpec(memory_space=pltpu.VMEM)
HBM = pl.BlockSpec(memory_space=pltpu.HBM)
NT = (((1,), (1,)), ((), ()))


def rope_tables(n_rows, head_dim):
    half = head_dim // 2
    quarter = half // 2
    inverse = ROPE_BASE ** (-np.arange(quarter, dtype=np.float64) * (2.0 / half))
    channel = np.arange(LANES) % head_dim
    freq = inverse[channel % quarter]
    sign = np.where(channel % half < quarter, -1.0, 1.0)
    by_row = channel < half

    def table(count, lanes):
        angles = np.arange(count, dtype=np.float64)[:, None] * freq[None, :]
        cosine = np.where(lanes[None, :], np.cos(angles), 0.0)
        sine = np.where(lanes[None, :], np.sin(angles) * sign[None, :], 0.0)
        return np.concatenate([cosine, sine], axis=1)

    pad = -n_rows % 8
    rows = np.concatenate([table(n_rows, by_row), np.zeros((pad, 2 * LANES))])
    return np.concatenate([table(GRID_W, ~by_row), rows]).astype(np.float32)


def turn(values, row_start, table_ref, head_dim):
    quarter = head_dim // 4
    rows = values.shape[0]
    lane = lax.broadcasted_iota(jnp.int32, (1, LANES), 1)
    ahead = pltpu.roll(values, LANES - quarter, 1)
    behind = pltpu.roll(values, quarter, 1)
    other = jnp.where(lane % (2 * quarter) < quarter, ahead, behind)
    columns = table_ref[0:GRID_W, :]
    out = []
    for j in range(rows // GRID_W):
        row = table_ref[pl.ds(GRID_W + row_start + j, 1), :]
        both = columns + row
        part = slice(j * GRID_W, (j + 1) * GRID_W)
        out.append(values[part] * both[:, :LANES] + other[part] * both[:, LANES:])
    return jnp.concatenate(out, axis=0)


def normed(values, gain, head_dim):
    lane = lax.broadcasted_iota(jnp.int32, (1, LANES), 1)
    gain = jnp.concatenate([gain] * (LANES // head_dim), axis=1)
    squares = values * values
    scale = jnp.zeros_like(values)
    for g in range(LANES // head_dim):
        mine = lane // head_dim == g
        mean = jnp.sum(jnp.where(mine, squares, 0.0), axis=1, keepdims=True) * (1.0 / head_dim)
        scale = jnp.where(mine, lax.rsqrt(mean + NORM_EPS), scale)
    return values * scale * gain


class Copies:
    def __init__(self, sems):
        self.sems = sems
        self.held = []

    def start(self, src, dst):
        copy = pltpu.make_async_copy(src, dst, self.sems.at[len(self.held)])
        copy.start()
        self.held.append(copy)

    def wait(self, first, last):
        for copy in self.held[first:last]:
            copy.wait()


def kv_kernel(
    head_dim, pieces, tok_hbm, wk_hbm, wv_hbm, gain_ref, table_hbm,
    out_ref, tok_ref, both_ref, table_ref, sems,
):
    rows, width = tok_ref.shape
    step = width // pieces
    copies = Copies(sems)
    for i in range(pieces):
        part = pl.ds(i * step, step)
        copies.start(tok_hbm.at[:, part], tok_ref.at[:, part])
        copies.start(wk_hbm.at[:, part], both_ref.at[pl.ds(0, head_dim), part])
        copies.start(wv_hbm.at[:, part], both_ref.at[pl.ds(head_dim, head_dim), part])
    copies.start(table_hbm.at[:, pl.ds(0, 2 * LANES)], table_ref)
    raw = None
    for i in range(pieces):
        copies.wait(3 * i, 3 * i + 3)
        part = slice(i * step, (i + 1) * step)
        more = lax.dot_general(
            tok_ref[:, part], both_ref[:, part], NT, preferred_element_type=jnp.float32
        )
        raw = more if raw is None else raw + more
    raw = raw.astype(jnp.bfloat16).astype(jnp.float32)
    lane = lax.broadcasted_iota(jnp.int32, (1, LANES), 1)
    row_start = lax.axis_index("sp") * (rows // GRID_W)
    copies.wait(3 * pieces, 3 * pieces + 1)
    keys = turn(normed(raw, gain_ref[...], head_dim), row_start, table_ref, head_dim)
    out_ref[...] = jnp.where(lane < head_dim, keys, raw).astype(jnp.bfloat16)


def attend(qt, kvs, head_dim, top, total, acc, score_ref, weight_ref):
    width = qt.shape[1]
    states = [] if top is None else [(top, total, acc)]
    at = 0
    for kv in kvs:
        count = kv.shape[0]
        score_ref[at : at + count, :] = jnp.dot(kv, qt, preferred_element_type=jnp.float32)
        eight = score_ref[at : at + 8, :]
        for i in range(8, count, 8):
            eight = jnp.maximum(eight, score_ref[at + i : at + i + 8, :])
        most = jnp.max(eight, axis=0, keepdims=True)
        part = jnp.zeros((8, width), jnp.float32)
        for i in range(at, at + count, 16):
            expos = jnp.exp(score_ref[i : i + 16, :] - most)
            weight_ref[i : i + 16, :] = expos.astype(jnp.bfloat16)
            part = part + (expos[:8] + expos[8:])
        values = kv.astype(jnp.float32).T[head_dim : 2 * head_dim].astype(jnp.bfloat16)
        weights = weight_ref[at : at + count, :]
        states.append((most, part, jnp.dot(values, weights, preferred_element_type=jnp.float32)))
        at += count
    if len(states) == 1:
        return states[0]
    top = functools.reduce(jnp.maximum, [state[0] for state in states])
    shrinks = [jnp.exp(state[0] - top) for state in states]
    total = sum(state[1] * shrink for state, shrink in zip(states, shrinks))
    acc = sum(state[2] * shrink for state, shrink in zip(states, shrinks))
    return top, total, acc


def attend_all(qt_ref, kv_refs, head_dim, state, score_ref, weight_ref):
    spare = head_dim, *state, score_ref, weight_ref
    if sum(kv_ref.shape[0] for kv_ref in kv_refs) <= SPAN:
        return attend(qt_ref[...], [kv_ref[...] for kv_ref in kv_refs], *spare)
    for kv_ref in kv_refs:
        length = kv_ref.shape[0]
        step = length
        while step > SPAN:
            step //= 2
        if length == step:
            state = attend(qt_ref[...], [kv_ref[...]], head_dim, *state, score_ref, weight_ref)
        else:

            def body(i, carry, kv_ref=kv_ref, step=step):
                at = pl.multiple_of(i * step, step)
                kvs = [kv_ref[pl.ds(at, step), :]]
                return attend(qt_ref[...], kvs, head_dim, *carry, score_ref, weight_ref)

            state = lax.fori_loop(0, length // step, body, state)
    return state


def q_kernel(head_dim, tok_ref, wq_ref, gain_ref, table_ref, qt_ref):
    rows = tok_ref.shape[0]
    heads = wq_ref.shape[1] // head_dim
    raw = jnp.dot(tok_ref[...], wq_ref[...], preferred_element_type=jnp.float32)
    raw = raw.astype(jnp.bfloat16).astype(jnp.float32)
    row_start = lax.axis_index("sp") * (rows // GRID_W)
    per = LANES // head_dim
    columns = []
    for p in range(heads // per):
        x = raw[:, p * LANES : (p + 1) * LANES]
        y = turn(normed(x, gain_ref[...], head_dim), row_start, table_ref, head_dim)
        yt = (y * (head_dim ** -0.5)).T
        columns += [yt[g * head_dim : (g + 1) * head_dim] for g in range(per)]
    qt = jnp.concatenate(columns, axis=1)
    qt = jnp.concatenate([qt, jnp.zeros((LANES - head_dim, qt.shape[1]), jnp.float32)], axis=0)
    qt_ref[...] = qt.astype(jnp.bfloat16)


def first_kernel(head_dim, qt_ref, *refs):
    kv_refs = refs[:-5]
    top_ref, total_ref, acc_ref, *spare = refs[-5:]
    state = attend_all(qt_ref, kv_refs, head_dim, (None, None, None), *spare)
    top_ref[...], total_ref[...], acc_ref[...] = state


def block_kernel(head_dim, qt_ref, *refs):
    kv_refs = refs[:-8]
    top_in, total_in, acc_in, top_ref, total_ref, acc_ref, *spare = refs[-8:]
    state = attend_all(qt_ref, kv_refs, head_dim, (top_in[...], total_in[...], acc_in[...]), *spare)
    top_ref[...], total_ref[...], acc_ref[...] = state


def finish_kernel(head_dim, qt_ref, *refs):
    kv_refs = refs[:-10]
    top_in, total_in, acc_in, wo_ref, att_ref, top_ref, sum_ref, sent_ref, *spare = refs[-10:]
    state = attend_all(qt_ref, kv_refs, head_dim, (top_in[...], total_in[...], acc_in[...]), *spare)
    top, total, acc = state
    summed = jnp.sum(total, axis=0, keepdims=True)
    out = acc * (1.0 / summed)
    rows = att_ref.shape[0]
    heads = top_ref.shape[0]
    per = LANES // head_dim
    for p in range(heads // per):
        pair = [out[:, h * rows : (h + 1) * rows] for h in range(p * per, (p + 1) * per)]
        att = jnp.concatenate(pair, axis=0).T
        att_ref[:, p * LANES : (p + 1) * LANES] = att.astype(jnp.bfloat16)
    own = sent_ref.shape[0]
    sent_ref[...] = product(att_ref, wo_ref, rows // own - 1, own).astype(jnp.bfloat16)
    for h in range(heads):
        top_ref[h : h + 1, :] = top[:, h * rows : (h + 1) * rows]
        sum_ref[h : h + 1, :] = summed[:, h * rows : (h + 1) * rows]


def product(att_ref, wo_ref, d, own):
    at = pl.multiple_of((lax.axis_index("tp") ^ d) * own, own)
    return jnp.dot(att_ref[pl.ds(at, own), :], wo_ref[...], preferred_element_type=jnp.float32)


def rest_kernel(att_ref, wo_ref, *out_refs):
    for d, out_ref in enumerate(out_refs):
        out = product(att_ref, wo_ref, d, out_ref.shape[0])
        out_ref[...] = out.astype(out_ref.dtype)


def call(kernel, out_shape, flops, in_specs, limit=LIMIT, **more):
    return pl.pallas_call(
        kernel,
        out_shape=out_shape,
        in_specs=in_specs,
        out_specs=jax.tree.map(lambda _: VMEM, out_shape),
        cost_estimate=pl.CostEstimate(flops=flops, bytes_accessed=flops // 256, transcendentals=0),
        compiler_params=pltpu.CompilerParams(vmem_limit_bytes=limit),
        **more,
    )


def xor(n, bit):
    return [(i, i ^ bit) for i in range(n)]


def shards(n_sp, n_tp, tokens, w_query, w_key, w_value, w_output, query_gain, key_gain):
    head_dim = query_gain.shape[0]
    rows, width = tokens.shape
    heads = w_query.shape[1] // head_dim
    table = rope_tables(n_sp * rows // GRID_W, head_dim)
    wide = jnp.asarray(np.pad(table, ((0, 0), (0, 7 * table.shape[1]))))
    table = jnp.asarray(table)
    f32 = functools.partial(jax.ShapeDtypeStruct, dtype=jnp.float32)
    bf16 = functools.partial(jax.ShapeDtypeStruct, dtype=jnp.bfloat16)
    pieces = 1

    scratch = [pltpu.VMEM((1, head_dim), jnp.float32), pltpu.VMEM((table.shape[0], 2 * LANES), jnp.float32)]
    kv = call(
        functools.partial(kv_kernel, head_dim, pieces),
        bf16((rows, LANES)),
        2 * rows * width * LANES,
        [HBM] * 3 + [VMEM, HBM],
        KV_LIMIT,
        scratch_shapes=[
            pltpu.VMEM(tokens.shape, jnp.bfloat16),
            pltpu.VMEM((LANES, width), jnp.bfloat16),
            scratch[1],
            pltpu.SemaphoreType.DMA((3 * pieces + 1,)),
        ],
    )(tokens, w_key.T, w_value.T, key_gain[None, :], wide)

    kv, tokens, w_query, w_output = lax.optimization_barrier((kv, tokens, w_query, w_output))
    size = heads * rows
    state_shape = [f32((1, size)), f32((8, size)), f32((head_dim, size))]

    def spare(kvs):
        count = min(SPAN, sum(x.shape[0] for x in kvs))
        return [pltpu.VMEM((count, size), jnp.float32), pltpu.VMEM((count, size), jnp.bfloat16)]

    def work(kvs):
        return sum(4 * size * x.shape[0] * LANES for x in kvs)

    qt = call(
        functools.partial(q_kernel, head_dim),
        bf16((LANES, size)),
        2 * rows * width * heads * head_dim,
        [VMEM] * 4,
    )(tokens, w_query, query_gain[None, :], table)

    def first(qt, *kvs):
        return call(
            functools.partial(first_kernel, head_dim),
            state_shape,
            work(kvs),
            [VMEM] * (1 + len(kvs)),
            scratch_shapes=spare(kvs),
        )(qt, *kvs)

    def blocks(qt, state, *kvs):
        return call(
            functools.partial(block_kernel, head_dim),
            state_shape,
            work(kvs),
            [VMEM] * (4 + len(kvs)),
            scratch_shapes=spare(kvs),
            input_output_aliases={1 + len(kvs) + i: i for i in range(3)},
        )(qt, *kvs, *state)

    own = rows // n_tp

    def finish(qt, state, *kvs):
        return call(
            functools.partial(finish_kernel, head_dim),
            [
                bf16((rows, heads * head_dim)),
                f32((heads, rows)),
                f32((heads, rows)),
                bf16((own, w_output.shape[1])),
            ],
            work(kvs),
            [VMEM] * (5 + len(kvs)),
            scratch_shapes=spare(kvs),
        )(qt, *kvs, *state, w_output)

    send = functools.partial(lax.ppermute, axis_name="sp")
    if n_sp == 8:
        near = send(kv, perm=xor(n_sp, 1))
        far = send(kv, perm=xor(n_sp, 4))
        pair = jnp.concatenate([kv, near], axis=0)
        middle = send(pair, perm=xor(n_sp, 6))
        beside = send(pair, perm=xor(n_sp, 2))
        relayed = send(far, perm=xor(n_sp, 1))
        state = first(qt, pair)
        state = blocks(qt, state, beside, far)
        attended, top, summed, sent = finish(qt, state, relayed, middle)
    else:
        held = kv
        state = None
        stride = 1
        pending = [kv]
        while stride < n_sp:
            radix = 2 if stride == 1 else min(4, n_sp // stride)
            got = [send(held, perm=xor(n_sp, d * stride)) for d in range(1, radix)]
            if state is None:
                state = first(qt, *pending)
            else:
                state = blocks(qt, state, *pending)
            pending = got
            stride *= radix
            if stride < n_sp:
                held = jnp.concatenate([held] + got, axis=0)
        attended, top, summed, sent = finish(qt, state, *pending)

    parts = call(
        rest_kernel,
        [(bf16 if d % 2 else f32)(sent.shape) for d in range(n_tp - 1)],
        2 * rows * w_output.size // n_tp,
        [VMEM] * 2,
    )(attended, w_output)
    parts = [*parts, sent]
    bit = 1
    while bit < n_tp:
        for d in reversed(range(0, n_tp, 2 * bit)):
            got = lax.ppermute(parts[d + bit].astype(jnp.bfloat16), "tp", xor(n_tp, bit))
            parts[d] = parts[d] + got.astype(jnp.float32)
        bit *= 2
    return parts[0].astype(jnp.bfloat16), top + jnp.log(summed)


def solution(mesh):
    placed = (P("sp", None), P(None, "tp"), P(None, "tp"), P(None, "tp"), P("tp", None), P(), P())
    return jax.shard_map(
        functools.partial(shards, mesh.shape["sp"], mesh.shape["tp"]),
        mesh=mesh,
        in_specs=placed,
        out_specs=(P(("sp", "tp"), None), P("tp", "sp")),
        check_vma=False,
    )
```

```python
import functools

import jax
import jax.numpy as jnp
import numpy as np
from jax import lax
from jax.experimental import pallas as pl
from jax.experimental.pallas import tpu as pltpu
from jax.sharding import PartitionSpec as P


GRID_W = 64
ROPE_BASE = 10000.0
NORM_EPS = 1e-06
LANES = 128
LIMIT = 12 << 20
SPAN = 768
KV_LIMIT = 56480000


VMEM = pl.BlockSpec(memory_space=pltpu.VMEM)
HBM = pl.BlockSpec(memory_space=pltpu.HBM)
NT = (((1,), (1,)), ((), ()))


def rope_tables(n_rows, head_dim):
    half = head_dim // 2
    quarter = half // 2
    inverse = ROPE_BASE ** (-np.arange(quarter, dtype=np.float64) * (2.0 / half))
    channel = np.arange(LANES) % head_dim
    freq = inverse[channel % quarter]
    sign = np.where(channel % half < quarter, -1.0, 1.0)
    by_row = channel < half

    def table(count, lanes):
        angles = np.arange(count, dtype=np.float64)[:, None] * freq[None, :]
        cosine = np.where(lanes[None, :], np.cos(angles), 0.0)
        sine = np.where(lanes[None, :], np.sin(angles) * sign[None, :], 0.0)
        return np.concatenate([cosine, sine], axis=1)

    pad = -n_rows % 8
    rows = np.concatenate([table(n_rows, by_row), np.zeros((pad, 2 * LANES))])
    return np.concatenate([table(GRID_W, ~by_row), rows]).astype(np.float32)


def turn(values, row_start, table_ref, head_dim):
    quarter = head_dim // 4
    rows = values.shape[0]
    lane = lax.broadcasted_iota(jnp.int32, (1, LANES), 1)
    ahead = pltpu.roll(values, LANES - quarter, 1)
    behind = pltpu.roll(values, quarter, 1)
    other = jnp.where(lane % (2 * quarter) < quarter, ahead, behind)
    columns = table_ref[0:GRID_W, :]
    out = []
    for j in range(rows // GRID_W):
        row = table_ref[pl.ds(GRID_W + row_start + j, 1), :]
        both = columns + row
        part = slice(j * GRID_W, (j + 1) * GRID_W)
        out.append(values[part] * both[:, :LANES] + other[part] * both[:, LANES:])
    return jnp.concatenate(out, axis=0)


def normed(values, gain, head_dim):
    lane = lax.broadcasted_iota(jnp.int32, (1, LANES), 1)
    gain = jnp.concatenate([gain] * (LANES // head_dim), axis=1)
    squares = values * values
    scale = jnp.zeros_like(values)
    for g in range(LANES // head_dim):
        mine = lane // head_dim == g
        mean = jnp.sum(jnp.where(mine, squares, 0.0), axis=1, keepdims=True) * (1.0 / head_dim)
        scale = jnp.where(mine, lax.rsqrt(mean + NORM_EPS), scale)
    return values * scale * gain


class Copies:
    def __init__(self, sems):
        self.sems = sems
        self.held = []

    def start(self, src, dst):
        copy = pltpu.make_async_copy(src, dst, self.sems.at[len(self.held)])
        copy.start()
        self.held.append(copy)

    def wait(self, first, last):
        for copy in self.held[first:last]:
            copy.wait()


def kv_kernel(
    head_dim, pieces, tok_hbm, wk_hbm, wv_hbm, gain_ref, table_hbm,
    out_ref, tok_ref, both_ref, table_ref, sems,
):
    rows, width = tok_ref.shape
    step = width // pieces
    copies = Copies(sems)
    for i in range(pieces):
        part = pl.ds(i * step, step)
        copies.start(tok_hbm.at[:, part], tok_ref.at[:, part])
        copies.start(wk_hbm.at[:, part], both_ref.at[pl.ds(0, head_dim), part])
        copies.start(wv_hbm.at[:, part], both_ref.at[pl.ds(head_dim, head_dim), part])
    copies.start(table_hbm.at[:, pl.ds(0, 2 * LANES)], table_ref)
    raw = None
    for i in range(pieces):
        copies.wait(3 * i, 3 * i + 3)
        part = slice(i * step, (i + 1) * step)
        more = lax.dot_general(
            tok_ref[:, part], both_ref[:, part], NT, preferred_element_type=jnp.float32
        )
        raw = more if raw is None else raw + more
    rounded = raw.astype(jnp.bfloat16)
    quarter = head_dim // 4
    source = lax.broadcasted_iota(jnp.int32, (LANES, LANES), 0)
    target = lax.broadcasted_iota(jnp.int32, (LANES, LANES), 1)
    step = jnp.where(target % (2 * quarter) < quarter, quarter, -quarter)
    swap = jnp.where(source == target + step, 1.0, 0.0).astype(jnp.bfloat16)
    other = jnp.dot(rounded, swap, preferred_element_type=jnp.float32)
    raw = rounded.astype(jnp.float32)
    lane = lax.broadcasted_iota(jnp.int32, (1, LANES), 1)
    mine = lane < head_dim
    mean = jnp.sum(jnp.where(mine, raw * raw, 0.0), axis=1, keepdims=True) * (1.0 / head_dim)
    scale = lax.rsqrt(mean + NORM_EPS)
    gain = jnp.concatenate([gain_ref[...]] * (LANES // head_dim), axis=1)
    ahead, behind = pltpu.roll(gain, LANES - quarter, 1), pltpu.roll(gain, quarter, 1)
    other_gain = jnp.where(lane % (2 * quarter) < quarter, ahead, behind)
    row_start = lax.axis_index("sp") * (rows // GRID_W)
    copies.wait(3 * pieces, 3 * pieces + 1)
    columns = table_ref[0:GRID_W, :]
    for j in range(rows // GRID_W):
        part = slice(j * GRID_W, (j + 1) * GRID_W)
        both = columns + table_ref[pl.ds(GRID_W + row_start + j, 1), :]
        keys = raw[part] * (gain * both[:, :LANES]) + other[part] * (other_gain * both[:, LANES:])
        out = jnp.where(mine, keys * scale[part], raw[part])
        out_ref[part, :] = out.astype(jnp.bfloat16)


def attend(qt, kvs, head_dim, top, total, acc, score_ref, weight_ref):
    width = qt.shape[1]
    states = [] if top is None else [(top, total, acc)]
    at = 0
    for kv in kvs:
        count = kv.shape[0]
        score_ref[at : at + count, :] = jnp.dot(kv, qt, preferred_element_type=jnp.float32)
        eight = score_ref[at : at + 8, :]
        for i in range(8, count, 8):
            eight = jnp.maximum(eight, score_ref[at + i : at + i + 8, :])
        most = jnp.max(eight, axis=0, keepdims=True)
        part = jnp.zeros((8, width), jnp.float32)
        for i in range(at, at + count, 16):
            expos = jnp.exp(score_ref[i : i + 16, :] - most)
            weight_ref[i : i + 16, :] = expos.astype(jnp.bfloat16)
            part = part + (expos[:8] + expos[8:])
        values = kv.astype(jnp.float32).T[head_dim : 2 * head_dim].astype(jnp.bfloat16)
        weights = weight_ref[at : at + count, :]
        states.append((most, part, jnp.dot(values, weights, preferred_element_type=jnp.float32)))
        at += count
    if len(states) == 1:
        return states[0]
    top = functools.reduce(jnp.maximum, [state[0] for state in states])
    shrinks = [jnp.exp(state[0] - top) for state in states]
    total = sum(state[1] * shrink for state, shrink in zip(states, shrinks))
    acc = sum(state[2] * shrink for state, shrink in zip(states, shrinks))
    return top, total, acc


def attend_all(qt_ref, kv_refs, head_dim, state, score_ref, weight_ref):
    spare = head_dim, *state, score_ref, weight_ref
    if sum(kv_ref.shape[0] for kv_ref in kv_refs) <= SPAN:
        return attend(qt_ref[...], [kv_ref[...] for kv_ref in kv_refs], *spare)
    for kv_ref in kv_refs:
        length = kv_ref.shape[0]
        step = length
        while step > SPAN:
            step //= 2
        if length == step:
            state = attend(qt_ref[...], [kv_ref[...]], head_dim, *state, score_ref, weight_ref)
        else:

            def body(i, carry, kv_ref=kv_ref, step=step):
                at = pl.multiple_of(i * step, step)
                kvs = [kv_ref[pl.ds(at, step), :]]
                return attend(qt_ref[...], kvs, head_dim, *carry, score_ref, weight_ref)

            state = lax.fori_loop(0, length // step, body, state)
    return state


def q_kernel(head_dim, tok_ref, wq_ref, gain_ref, table_ref, qt_ref):
    rows = tok_ref.shape[0]
    heads = wq_ref.shape[1] // head_dim
    raw = jnp.dot(tok_ref[...], wq_ref[...], preferred_element_type=jnp.float32)
    raw = raw.astype(jnp.bfloat16).astype(jnp.float32)
    row_start = lax.axis_index("sp") * (rows // GRID_W)
    per = LANES // head_dim
    columns = []
    for p in range(heads // per):
        x = raw[:, p * LANES : (p + 1) * LANES]
        y = turn(normed(x, gain_ref[...], head_dim), row_start, table_ref, head_dim)
        yt = (y * (head_dim ** -0.5)).T
        columns += [yt[g * head_dim : (g + 1) * head_dim] for g in range(per)]
    qt = jnp.concatenate(columns, axis=1)
    qt = jnp.concatenate([qt, jnp.zeros((LANES - head_dim, qt.shape[1]), jnp.float32)], axis=0)
    qt_ref[...] = qt.astype(jnp.bfloat16)


def first_kernel(head_dim, qt_ref, *refs):
    kv_refs = refs[:-5]
    top_ref, total_ref, acc_ref, *spare = refs[-5:]
    state = attend_all(qt_ref, kv_refs, head_dim, (None, None, None), *spare)
    top_ref[...], total_ref[...], acc_ref[...] = state


def block_kernel(head_dim, qt_ref, *refs):
    kv_refs = refs[:-8]
    top_in, total_in, acc_in, top_ref, total_ref, acc_ref, *spare = refs[-8:]
    state = attend_all(qt_ref, kv_refs, head_dim, (top_in[...], total_in[...], acc_in[...]), *spare)
    top_ref[...], total_ref[...], acc_ref[...] = state


def finish_kernel(head_dim, qt_ref, *refs):
    kv_refs = refs[:-10]
    top_in, total_in, acc_in, wo_ref, att_ref, top_ref, sum_ref, sent_ref, *spare = refs[-10:]
    state = attend_all(qt_ref, kv_refs, head_dim, (top_in[...], total_in[...], acc_in[...]), *spare)
    top, total, acc = state
    summed = jnp.sum(total, axis=0, keepdims=True)
    out = acc * (1.0 / summed)
    rows = att_ref.shape[0]
    heads = top_ref.shape[0]
    per = LANES // head_dim
    for p in range(heads // per):
        pair = [out[:, h * rows : (h + 1) * rows] for h in range(p * per, (p + 1) * per)]
        att = jnp.concatenate(pair, axis=0).T
        att_ref[:, p * LANES : (p + 1) * LANES] = att.astype(jnp.bfloat16)
    own = sent_ref.shape[0]
    sent_ref[...] = product(att_ref, wo_ref, rows // own - 1, own).astype(jnp.bfloat16)
    for h in range(heads):
        top_ref[h : h + 1, :] = top[:, h * rows : (h + 1) * rows]
        sum_ref[h : h + 1, :] = summed[:, h * rows : (h + 1) * rows]


def product(att_ref, wo_ref, d, own):
    at = pl.multiple_of((lax.axis_index("tp") ^ d) * own, own)
    return jnp.dot(att_ref[pl.ds(at, own), :], wo_ref[...], preferred_element_type=jnp.float32)


def rest_kernel(att_ref, wo_ref, *out_refs):
    for d, out_ref in enumerate(out_refs):
        out = product(att_ref, wo_ref, d, out_ref.shape[0])
        out_ref[...] = out.astype(out_ref.dtype)


def call(kernel, out_shape, flops, in_specs, limit=LIMIT, **more):
    return pl.pallas_call(
        kernel,
        out_shape=out_shape,
        in_specs=in_specs,
        out_specs=jax.tree.map(lambda _: VMEM, out_shape),
        cost_estimate=pl.CostEstimate(flops=flops, bytes_accessed=flops // 256, transcendentals=0),
        compiler_params=pltpu.CompilerParams(vmem_limit_bytes=limit),
        **more,
    )


def xor(n, bit):
    return [(i, i ^ bit) for i in range(n)]


def shards(n_sp, n_tp, tokens, w_query, w_key, w_value, w_output, query_gain, key_gain):
    head_dim = query_gain.shape[0]
    rows, width = tokens.shape
    heads = w_query.shape[1] // head_dim
    table = rope_tables(n_sp * rows // GRID_W, head_dim)
    wide = jnp.asarray(np.pad(table, ((0, 0), (0, 7 * table.shape[1]))))
    table = jnp.asarray(table)
    f32 = functools.partial(jax.ShapeDtypeStruct, dtype=jnp.float32)
    bf16 = functools.partial(jax.ShapeDtypeStruct, dtype=jnp.bfloat16)
    pieces = 1

    scratch = [pltpu.VMEM((1, head_dim), jnp.float32), pltpu.VMEM((table.shape[0], 2 * LANES), jnp.float32)]
    kv = call(
        functools.partial(kv_kernel, head_dim, pieces),
        bf16((rows, LANES)),
        2 * rows * width * LANES,
        [HBM] * 3 + [VMEM, HBM],
        KV_LIMIT,
        scratch_shapes=[
            pltpu.VMEM(tokens.shape, jnp.bfloat16),
            pltpu.VMEM((LANES, width), jnp.bfloat16),
            scratch[1],
            pltpu.SemaphoreType.DMA((3 * pieces + 1,)),
        ],
    )(tokens, w_key.T, w_value.T, key_gain[None, :], wide)

    kv, tokens, w_query, w_output = lax.optimization_barrier((kv, tokens, w_query, w_output))
    size = heads * rows
    state_shape = [f32((1, size)), f32((8, size)), f32((head_dim, size))]

    def spare(kvs):
        count = min(SPAN, sum(x.shape[0] for x in kvs))
        return [pltpu.VMEM((count, size), jnp.float32), pltpu.VMEM((count, size), jnp.bfloat16)]

    def work(kvs):
        return sum(4 * size * x.shape[0] * LANES for x in kvs)

    qt = call(
        functools.partial(q_kernel, head_dim),
        bf16((LANES, size)),
        2 * rows * width * heads * head_dim,
        [VMEM] * 4,
    )(tokens, w_query, query_gain[None, :], table)

    def first(qt, *kvs):
        return call(
            functools.partial(first_kernel, head_dim),
            state_shape,
            work(kvs),
            [VMEM] * (1 + len(kvs)),
            scratch_shapes=spare(kvs),
        )(qt, *kvs)

    def blocks(qt, state, *kvs):
        return call(
            functools.partial(block_kernel, head_dim),
            state_shape,
            work(kvs),
            [VMEM] * (4 + len(kvs)),
            scratch_shapes=spare(kvs),
            input_output_aliases={1 + len(kvs) + i: i for i in range(3)},
        )(qt, *kvs, *state)

    own = rows // n_tp

    def finish(qt, state, *kvs):
        return call(
            functools.partial(finish_kernel, head_dim),
            [
                bf16((rows, heads * head_dim)),
                f32((heads, rows)),
                f32((heads, rows)),
                bf16((own, w_output.shape[1])),
            ],
            work(kvs),
            [VMEM] * (5 + len(kvs)),
            scratch_shapes=spare(kvs),
        )(qt, *kvs, *state, w_output)

    send = functools.partial(lax.ppermute, axis_name="sp")
    if n_sp == 8:
        near = send(kv, perm=xor(n_sp, 1))
        far = send(kv, perm=xor(n_sp, 4))
        pair = jnp.concatenate([kv, near], axis=0)
        middle = send(pair, perm=xor(n_sp, 6))
        beside = send(pair, perm=xor(n_sp, 2))
        relayed = send(far, perm=xor(n_sp, 1))
        state = first(qt, pair)
        state = blocks(qt, state, beside, far)
        attended, top, summed, sent = finish(qt, state, relayed, middle)
    else:
        held = kv
        state = None
        stride = 1
        pending = [kv]
        while stride < n_sp:
            radix = 2 if stride == 1 else min(4, n_sp // stride)
            got = [send(held, perm=xor(n_sp, d * stride)) for d in range(1, radix)]
            if state is None:
                state = first(qt, *pending)
            else:
                state = blocks(qt, state, *pending)
            pending = got
            stride *= radix
            if stride < n_sp:
                held = jnp.concatenate([held] + got, axis=0)
        attended, top, summed, sent = finish(qt, state, *pending)

    parts = call(
        rest_kernel,
        [(bf16 if d % 2 else f32)(sent.shape) for d in range(n_tp - 1)],
        2 * rows * w_output.size // n_tp,
        [VMEM] * 2,
    )(attended, w_output)
    parts = [*parts, sent]
    bit = 1
    while bit < n_tp:
        for d in reversed(range(0, n_tp, 2 * bit)):
            got = lax.ppermute(parts[d + bit].astype(jnp.bfloat16), "tp", xor(n_tp, bit))
            parts[d] = parts[d] + got.astype(jnp.float32)
        bit *= 2
    return parts[0].astype(jnp.bfloat16), top + jnp.log(summed)


def solution(mesh):
    placed = (P("sp", None), P(None, "tp"), P(None, "tp"), P(None, "tp"), P("tp", None), P(), P())
    return jax.shard_map(
        functools.partial(shards, mesh.shape["sp"], mesh.shape["tp"]),
        mesh=mesh,
        in_specs=placed,
        out_specs=(P(("sp", "tp"), None), P("tp", "sp")),
        check_vma=False,
    )
```

```python
import functools

import jax
import jax.numpy as jnp
import numpy as np
from jax import lax
from jax.experimental import pallas as pl
from jax.experimental.pallas import tpu as pltpu
from jax.sharding import PartitionSpec as P


GRID_W = 64
ROPE_BASE = 10000.0
NORM_EPS = 1e-06
LANES = 128
LIMIT = 12 << 20
SPAN = 1024
KV_LIMIT = 56480000


VMEM = pl.BlockSpec(memory_space=pltpu.VMEM)
HBM = pl.BlockSpec(memory_space=pltpu.HBM)
NT = (((1,), (1,)), ((), ()))


def rope_tables(n_rows, head_dim):
    half = head_dim // 2
    quarter = half // 2
    inverse = ROPE_BASE ** (-np.arange(quarter, dtype=np.float64) * (2.0 / half))
    channel = np.arange(LANES) % head_dim
    freq = inverse[channel % quarter]
    sign = np.where(channel % half < quarter, -1.0, 1.0)
    by_row = channel < half

    def table(count, lanes):
        angles = np.arange(count, dtype=np.float64)[:, None] * freq[None, :]
        cosine = np.where(lanes[None, :], np.cos(angles), 0.0)
        sine = np.where(lanes[None, :], np.sin(angles) * sign[None, :], 0.0)
        return np.concatenate([cosine, sine], axis=1)

    pad = -n_rows % 8
    rows = np.concatenate([table(n_rows, by_row), np.zeros((pad, 2 * LANES))])
    return np.concatenate([table(GRID_W, ~by_row), rows]).astype(np.float32)


def swap_matrix(head_dim):
    quarter = head_dim // 4
    source = lax.broadcasted_iota(jnp.int32, (LANES, LANES), 0)
    target = lax.broadcasted_iota(jnp.int32, (LANES, LANES), 1)
    step = jnp.where(target % (2 * quarter) < quarter, quarter, -quarter)
    return jnp.where(source == target + step, 1.0, 0.0).astype(jnp.bfloat16)


def swapped(row, head_dim):
    quarter = head_dim // 4
    lane = lax.broadcasted_iota(jnp.int32, (1, LANES), 1)
    ahead, behind = pltpu.roll(row, LANES - quarter, 1), pltpu.roll(row, quarter, 1)
    return jnp.where(lane % (2 * quarter) < quarter, ahead, behind)


class Copies:
    def __init__(self, sems):
        self.sems = sems
        self.held = []

    def start(self, src, dst):
        copy = pltpu.make_async_copy(src, dst, self.sems.at[len(self.held)])
        copy.start()
        self.held.append(copy)

    def wait(self, first, last):
        for copy in self.held[first:last]:
            copy.wait()


def kv_kernel(
    head_dim, pieces, tok_hbm, wk_hbm, wv_hbm, gain_ref, table_hbm,
    out_ref, tok_ref, both_ref, table_ref, sems,
):
    rows, width = tok_ref.shape
    step = width // pieces
    copies = Copies(sems)
    for i in range(pieces):
        part = pl.ds(i * step, step)
        copies.start(tok_hbm.at[:, part], tok_ref.at[:, part])
        copies.start(wk_hbm.at[:, part], both_ref.at[pl.ds(0, head_dim), part])
        copies.start(wv_hbm.at[:, part], both_ref.at[pl.ds(head_dim, head_dim), part])
    copies.start(table_hbm.at[:, pl.ds(0, 2 * LANES)], table_ref)
    raw = None
    for i in range(pieces):
        copies.wait(3 * i, 3 * i + 3)
        part = slice(i * step, (i + 1) * step)
        more = lax.dot_general(
            tok_ref[:, part], both_ref[:, part], NT, preferred_element_type=jnp.float32
        )
        raw = more if raw is None else raw + more
    rounded = raw.astype(jnp.bfloat16)
    swap = swap_matrix(head_dim)
    other = jnp.dot(rounded, swap, preferred_element_type=jnp.float32)
    raw = rounded.astype(jnp.float32)
    lane = lax.broadcasted_iota(jnp.int32, (1, LANES), 1)
    mine = lane < head_dim
    mean = jnp.sum(jnp.where(mine, raw * raw, 0.0), axis=1, keepdims=True) * (1.0 / head_dim)
    scale = lax.rsqrt(mean + NORM_EPS)
    gain = jnp.concatenate([gain_ref[...]] * (LANES // head_dim), axis=1)
    other_gain = swapped(gain, head_dim)
    row_start = lax.axis_index("sp") * (rows // GRID_W)
    copies.wait(3 * pieces, 3 * pieces + 1)
    columns = table_ref[0:GRID_W, :]
    for j in range(rows // GRID_W):
        part = slice(j * GRID_W, (j + 1) * GRID_W)
        both = columns + table_ref[pl.ds(GRID_W + row_start + j, 1), :]
        keys = raw[part] * (gain * both[:, :LANES]) + other[part] * (other_gain * both[:, LANES:])
        out = jnp.where(mine, keys * scale[part], raw[part])
        out_ref[part, :] = out.astype(jnp.bfloat16)


def attend(qt, kvs, head_dim, top, total, acc, score_ref, weight_ref):
    width = qt.shape[1]
    states = [] if top is None else [(top, total, acc)]
    at = 0
    for kv in kvs:
        count = kv.shape[0]
        score_ref[at : at + count, :] = jnp.dot(kv, qt, preferred_element_type=jnp.float32)
        eight = score_ref[at : at + 8, :]
        for i in range(8, count, 8):
            eight = jnp.maximum(eight, score_ref[at + i : at + i + 8, :])
        most = jnp.max(eight, axis=0, keepdims=True)
        part = jnp.zeros((8, width), jnp.float32)
        for i in range(at, at + count, 16):
            expos = jnp.exp(score_ref[i : i + 16, :] - most)
            weight_ref[i : i + 16, :] = expos.astype(jnp.bfloat16)
            part = part + (expos[:8] + expos[8:])
        values = kv.astype(jnp.float32).T[head_dim : 2 * head_dim].astype(jnp.bfloat16)
        weights = weight_ref[at : at + count, :]
        states.append((most, part, jnp.dot(values, weights, preferred_element_type=jnp.float32)))
        at += count
    if len(states) == 1:
        return states[0]
    top = functools.reduce(jnp.maximum, [state[0] for state in states])
    shrinks = [jnp.exp(state[0] - top) for state in states]
    total = sum(state[1] * shrink for state, shrink in zip(states, shrinks))
    acc = sum(state[2] * shrink for state, shrink in zip(states, shrinks))
    return top, total, acc


def attend_all(qt_ref, kv_refs, head_dim, state, score_ref, weight_ref):
    spare = head_dim, *state, score_ref, weight_ref
    if sum(kv_ref.shape[0] for kv_ref in kv_refs) <= SPAN:
        return attend(qt_ref[...], [kv_ref[...] for kv_ref in kv_refs], *spare)
    for kv_ref in kv_refs:
        length = kv_ref.shape[0]
        step = length
        while step > SPAN:
            step //= 2
        if length == step:
            state = attend(qt_ref[...], [kv_ref[...]], head_dim, *state, score_ref, weight_ref)
        else:

            def body(i, carry, kv_ref=kv_ref, step=step):
                at = pl.multiple_of(i * step, step)
                kvs = [kv_ref[pl.ds(at, step), :]]
                return attend(qt_ref[...], kvs, head_dim, *carry, score_ref, weight_ref)

            state = lax.fori_loop(0, length // step, body, state)
    return state


def q_kernel(head_dim, tok_ref, wq_ref, gain_ref, table_ref, *refs):
    kv_refs = refs[:-6]
    qt_ref, top_ref, total_ref, acc_ref, *spare = refs[-6:]
    rows = tok_ref.shape[0]
    heads = wq_ref.shape[1] // head_dim
    raw = jnp.dot(tok_ref[...], wq_ref[...], preferred_element_type=jnp.float32)
    rounded = raw.astype(jnp.bfloat16)
    row_start = lax.axis_index("sp") * (rows // GRID_W)
    per = LANES // head_dim
    lane = lax.broadcasted_iota(jnp.int32, (1, LANES), 1)
    gain = jnp.concatenate([gain_ref[...]] * per, axis=1) * (head_dim ** -0.5)
    other_gain = swapped(gain, head_dim)
    swap = swap_matrix(head_dim)
    turns = []
    for j in range(rows // GRID_W):
        both = table_ref[0:GRID_W, :] + table_ref[pl.ds(GRID_W + row_start + j, 1), :]
        turns.append((gain * both[:, :LANES], other_gain * both[:, LANES:]))
    columns = []
    for p in range(heads // per):
        part = rounded[:, p * LANES : (p + 1) * LANES]
        other = jnp.dot(part, swap, preferred_element_type=jnp.float32)
        x = part.astype(jnp.float32)
        squares = x * x
        scale = None
        for g in range(per):
            mine = lane // head_dim == g
            mean = jnp.sum(jnp.where(mine, squares, 0.0), axis=1, keepdims=True) * (1.0 / head_dim)
            own = lax.rsqrt(mean + NORM_EPS)
            scale = own if scale is None else jnp.where(mine, own, scale)
        y = []
        for j, (cosine, sine) in enumerate(turns):
            some = slice(j * GRID_W, (j + 1) * GRID_W)
            y.append((x[some] * cosine + other[some] * sine) * scale[some])
        yt = jnp.concatenate(y, axis=0).T
        columns += [yt[g * head_dim : (g + 1) * head_dim] for g in range(per)]
    qt = jnp.concatenate(columns, axis=1)
    qt = jnp.concatenate([qt, jnp.zeros((LANES - head_dim, qt.shape[1]), jnp.float32)], axis=0)
    qt_ref[...] = qt.astype(jnp.bfloat16)
    state = attend_all(qt_ref, kv_refs, head_dim, (None, None, None), *spare)
    top_ref[...], total_ref[...], acc_ref[...] = state


def block_kernel(head_dim, qt_ref, *refs):
    kv_refs = refs[:-8]
    top_in, total_in, acc_in, top_ref, total_ref, acc_ref, *spare = refs[-8:]
    state = attend_all(qt_ref, kv_refs, head_dim, (top_in[...], total_in[...], acc_in[...]), *spare)
    top_ref[...], total_ref[...], acc_ref[...] = state


def finish_kernel(head_dim, qt_ref, *refs):
    kv_refs = refs[:-10]
    top_in, total_in, acc_in, wo_ref, att_ref, top_ref, sum_ref, sent_ref, *spare = refs[-10:]
    state = attend_all(qt_ref, kv_refs, head_dim, (top_in[...], total_in[...], acc_in[...]), *spare)
    top, total, acc = state
    summed = jnp.sum(total, axis=0, keepdims=True)
    out = acc * (1.0 / summed)
    rows = att_ref.shape[0]
    heads = top_ref.shape[0]
    per = LANES // head_dim
    for p in range(heads // per):
        pair = [out[:, h * rows : (h + 1) * rows] for h in range(p * per, (p + 1) * per)]
        att = jnp.concatenate(pair, axis=0).T
        att_ref[:, p * LANES : (p + 1) * LANES] = att.astype(jnp.bfloat16)
    own = sent_ref.shape[0]
    sent_ref[...] = product(att_ref, wo_ref, rows // own - 1, own).astype(jnp.bfloat16)
    for h in range(heads):
        top_ref[h : h + 1, :] = top[:, h * rows : (h + 1) * rows]
        sum_ref[h : h + 1, :] = summed[:, h * rows : (h + 1) * rows]


def product(att_ref, wo_ref, d, own):
    at = pl.multiple_of((lax.axis_index("tp") ^ d) * own, own)
    return jnp.dot(att_ref[pl.ds(at, own), :], wo_ref[...], preferred_element_type=jnp.float32)


def rest_kernel(att_ref, wo_ref, *out_refs):
    for d, out_ref in enumerate(out_refs):
        out = product(att_ref, wo_ref, d, out_ref.shape[0])
        out_ref[...] = out.astype(out_ref.dtype)


def call(kernel, out_shape, flops, in_specs, limit=LIMIT, **more):
    return pl.pallas_call(
        kernel,
        out_shape=out_shape,
        in_specs=in_specs,
        out_specs=jax.tree.map(lambda _: VMEM, out_shape),
        cost_estimate=pl.CostEstimate(flops=flops, bytes_accessed=flops // 256, transcendentals=0),
        compiler_params=pltpu.CompilerParams(vmem_limit_bytes=limit),
        **more,
    )


def xor(n, bit):
    return [(i, i ^ bit) for i in range(n)]


def shards(n_sp, n_tp, tokens, w_query, w_key, w_value, w_output, query_gain, key_gain):
    head_dim = query_gain.shape[0]
    rows, width = tokens.shape
    heads = w_query.shape[1] // head_dim
    table = rope_tables(n_sp * rows // GRID_W, head_dim)
    wide = jnp.asarray(np.pad(table, ((0, 0), (0, 7 * table.shape[1]))))
    table = jnp.asarray(table)
    f32 = functools.partial(jax.ShapeDtypeStruct, dtype=jnp.float32)
    bf16 = functools.partial(jax.ShapeDtypeStruct, dtype=jnp.bfloat16)
    pieces = 1

    scratch = [pltpu.VMEM((1, head_dim), jnp.float32), pltpu.VMEM((table.shape[0], 2 * LANES), jnp.float32)]
    kv = call(
        functools.partial(kv_kernel, head_dim, pieces),
        bf16((rows, LANES)),
        2 * rows * width * LANES,
        [HBM] * 3 + [VMEM, HBM],
        KV_LIMIT,
        scratch_shapes=[
            pltpu.VMEM(tokens.shape, jnp.bfloat16),
            pltpu.VMEM((LANES, width), jnp.bfloat16),
            scratch[1],
            pltpu.SemaphoreType.DMA((3 * pieces + 1,)),
        ],
    )(tokens, w_key.T, w_value.T, key_gain[None, :], wide)

    kv, tokens, w_query, w_output = lax.optimization_barrier((kv, tokens, w_query, w_output))
    size = heads * rows
    state_shape = [f32((1, size)), f32((8, size)), f32((head_dim, size))]

    def spare(kvs):
        count = min(SPAN, sum(x.shape[0] for x in kvs))
        return [pltpu.VMEM((count, size), jnp.float32), pltpu.VMEM((count, size), jnp.bfloat16)]

    def work(kvs):
        return sum(4 * size * x.shape[0] * LANES for x in kvs)

    def first(*kvs):
        qt, *state = call(
            functools.partial(q_kernel, head_dim),
            [bf16((LANES, size))] + state_shape,
            2 * rows * width * heads * head_dim + work(kvs),
            [VMEM] * (4 + len(kvs)),
            scratch_shapes=spare(kvs),
        )(tokens, w_query, query_gain[None, :], table, *kvs)
        return qt, state

    def blocks(qt, state, *kvs):
        return call(
            functools.partial(block_kernel, head_dim),
            state_shape,
            work(kvs),
            [VMEM] * (4 + len(kvs)),
            scratch_shapes=spare(kvs),
            input_output_aliases={1 + len(kvs) + i: i for i in range(3)},
        )(qt, *kvs, *state)

    own = rows // n_tp

    def finish(qt, state, *kvs):
        return call(
            functools.partial(finish_kernel, head_dim),
            [
                bf16((rows, heads * head_dim)),
                f32((heads, rows)),
                f32((heads, rows)),
                bf16((own, w_output.shape[1])),
            ],
            work(kvs),
            [VMEM] * (5 + len(kvs)),
            scratch_shapes=spare(kvs),
        )(qt, *kvs, *state, w_output)

    send = functools.partial(lax.ppermute, axis_name="sp")
    if n_sp == 8:
        near = send(kv, perm=xor(n_sp, 1))
        far = send(kv, perm=xor(n_sp, 4))
        pair = jnp.concatenate([kv, near], axis=0)
        middle = send(pair, perm=xor(n_sp, 6))
        beside = send(pair, perm=xor(n_sp, 2))
        relayed = send(far, perm=xor(n_sp, 1))
        qt, state = first(pair, beside, far)
        attended, top, summed, sent = finish(qt, state, relayed, middle)
    else:
        held = kv
        state = None
        stride = 1
        pending = [kv]
        while stride < n_sp:
            radix = 2 if stride == 1 else min(4, n_sp // stride)
            got = [send(held, perm=xor(n_sp, d * stride)) for d in range(1, radix)]
            if state is None:
                qt, state = first(*pending)
            else:
                state = blocks(qt, state, *pending)
            pending = got
            stride *= radix
            if stride < n_sp:
                held = jnp.concatenate([held] + got, axis=0)
        attended, top, summed, sent = finish(qt, state, *pending)

    parts = call(
        rest_kernel,
        [(bf16 if d % 2 else f32)(sent.shape) for d in range(n_tp - 1)],
        2 * rows * w_output.size // n_tp,
        [VMEM] * 2,
    )(attended, w_output)
    parts = [*parts, sent]
    bit = 1
    while bit < n_tp:
        for d in reversed(range(0, n_tp, 2 * bit)):
            got = lax.ppermute(parts[d + bit].astype(jnp.bfloat16), "tp", xor(n_tp, bit))
            parts[d] = parts[d] + got.astype(jnp.float32)
        bit *= 2
    return parts[0].astype(jnp.bfloat16), top + jnp.log(summed)


def solution(mesh):
    placed = (P("sp", None), P(None, "tp"), P(None, "tp"), P(None, "tp"), P("tp", None), P(), P())
    return jax.shard_map(
        functools.partial(shards, mesh.shape["sp"], mesh.shape["tp"]),
        mesh=mesh,
        in_specs=placed,
        out_specs=(P(("sp", "tp"), None), P("tp", "sp")),
        check_vma=False,
    )
```

```python
import functools

import jax
import jax.numpy as jnp
import numpy as np
from jax import lax
from jax.experimental import pallas as pl
from jax.experimental.pallas import tpu as pltpu
from jax.sharding import PartitionSpec as P


GRID_W = 64
ROPE_BASE = 10000.0
NORM_EPS = 1e-06
LANES = 128
LIMIT = 12 << 20
SPAN = 1024
KV_LIMIT = 56480000


VMEM = pl.BlockSpec(memory_space=pltpu.VMEM)
HBM = pl.BlockSpec(memory_space=pltpu.HBM)
NT = (((1,), (1,)), ((), ()))


def rope_tables(n_rows, head_dim):
    half = head_dim // 2
    quarter = half // 2
    inverse = ROPE_BASE ** (-np.arange(quarter, dtype=np.float64) * (2.0 / half))
    channel = np.arange(LANES) % head_dim
    freq = inverse[channel % quarter]
    sign = np.where(channel % half < quarter, -1.0, 1.0)
    by_row = channel < half

    def table(count, lanes):
        angles = np.arange(count, dtype=np.float64)[:, None] * freq[None, :]
        cosine = np.where(lanes[None, :], np.cos(angles), 0.0)
        sine = np.where(lanes[None, :], np.sin(angles) * sign[None, :], 0.0)
        return np.concatenate([cosine, sine], axis=1)

    pad = -n_rows % 8
    rows = np.concatenate([table(n_rows, by_row), np.zeros((pad, 2 * LANES))])
    return np.concatenate([table(GRID_W, ~by_row), rows]).astype(np.float32)


def swap_matrix(head_dim):
    quarter = head_dim // 4
    source = lax.broadcasted_iota(jnp.int32, (LANES, LANES), 0)
    target = lax.broadcasted_iota(jnp.int32, (LANES, LANES), 1)
    step = jnp.where(target % (2 * quarter) < quarter, quarter, -quarter)
    return jnp.where(source == target + step, 1.0, 0.0).astype(jnp.bfloat16)


def swapped(row, head_dim):
    quarter = head_dim // 4
    lane = lax.broadcasted_iota(jnp.int32, (1, LANES), 1)
    ahead, behind = pltpu.roll(row, LANES - quarter, 1), pltpu.roll(row, quarter, 1)
    return jnp.where(lane % (2 * quarter) < quarter, ahead, behind)


class Copies:
    def __init__(self, sems):
        self.sems = sems
        self.held = []

    def start(self, src, dst):
        copy = pltpu.make_async_copy(src, dst, self.sems.at[len(self.held)])
        copy.start()
        self.held.append(copy)

    def wait(self, first, last):
        for copy in self.held[first:last]:
            copy.wait()


def kv_kernel(
    head_dim, tok_hbm, wk_hbm, wv_hbm, gain_ref, table_hbm,
    out_ref, tok_ref, both_ref, table_ref, sems,
):
    rows, _ = tok_ref.shape
    copies = Copies(sems)
    copies.start(table_hbm.at[:, pl.ds(0, 2 * LANES)], table_ref)
    copies.start(wk_hbm, both_ref.at[pl.ds(0, head_dim)])
    copies.start(wv_hbm, both_ref.at[pl.ds(head_dim, head_dim)])
    copies.start(tok_hbm, tok_ref)
    swap = swap_matrix(head_dim)
    lane = lax.broadcasted_iota(jnp.int32, (1, LANES), 1)
    mine = lane < head_dim
    gain = jnp.concatenate([gain_ref[...]] * (LANES // head_dim), axis=1)
    other_gain = swapped(gain, head_dim)
    row_start = lax.axis_index("sp") * (rows // GRID_W)
    copies.wait(0, 1)
    turns = []
    for j in range(rows // GRID_W):
        both = table_ref[0:GRID_W, :] + table_ref[pl.ds(GRID_W + row_start + j, 1), :]
        turns.append((gain * both[:, :LANES], other_gain * both[:, LANES:]))
    copies.wait(1, 4)
    raw = lax.dot_general(tok_ref[...], both_ref[...], NT, preferred_element_type=jnp.float32)
    rounded = raw.astype(jnp.bfloat16)
    other = jnp.dot(rounded, swap, preferred_element_type=jnp.float32)
    raw = rounded.astype(jnp.float32)
    mean = jnp.sum(jnp.where(mine, raw * raw, 0.0), axis=1, keepdims=True) * (1.0 / head_dim)
    scale = lax.rsqrt(mean + NORM_EPS)
    for j, (cosine, sine) in enumerate(turns):
        part = slice(j * GRID_W, (j + 1) * GRID_W)
        keys = raw[part] * cosine + other[part] * sine
        out = jnp.where(mine, keys * scale[part], raw[part])
        out_ref[part, :] = out.astype(jnp.bfloat16)


def attend(qt, kvs, head_dim, top, total, acc, score_ref, weight_ref):
    width = qt.shape[1]
    states = [] if top is None else [(top, total, acc)]
    at = 0
    for kv in kvs:
        count = kv.shape[0]
        score_ref[at : at + count, :] = jnp.dot(kv, qt, preferred_element_type=jnp.float32)
        eight = score_ref[at : at + 8, :]
        for i in range(8, count, 8):
            eight = jnp.maximum(eight, score_ref[at + i : at + i + 8, :])
        most = jnp.max(eight, axis=0, keepdims=True)
        part = jnp.zeros((8, width), jnp.float32)
        for i in range(at, at + count, 16):
            expos = jnp.exp(score_ref[i : i + 16, :] - most)
            weight_ref[i : i + 16, :] = expos.astype(jnp.bfloat16)
            part = part + (expos[:8] + expos[8:])
        values = kv.astype(jnp.float32).T[head_dim : 2 * head_dim].astype(jnp.bfloat16)
        weights = weight_ref[at : at + count, :]
        states.append((most, part, jnp.dot(values, weights, preferred_element_type=jnp.float32)))
        at += count
    if len(states) == 1:
        return states[0]
    top = functools.reduce(jnp.maximum, [state[0] for state in states])
    shrinks = [jnp.exp(state[0] - top) for state in states]
    total = sum(state[1] * shrink for state, shrink in zip(states, shrinks))
    acc = sum(state[2] * shrink for state, shrink in zip(states, shrinks))
    return top, total, acc


def attend_all(qt_ref, kv_refs, head_dim, state, score_ref, weight_ref):
    spare = head_dim, *state, score_ref, weight_ref
    if sum(kv_ref.shape[0] for kv_ref in kv_refs) <= SPAN:
        return attend(qt_ref[...], [kv_ref[...] for kv_ref in kv_refs], *spare)
    for kv_ref in kv_refs:
        length = kv_ref.shape[0]
        step = length
        while step > SPAN:
            step //= 2
        if length == step:
            state = attend(qt_ref[...], [kv_ref[...]], head_dim, *state, score_ref, weight_ref)
        else:

            def body(i, carry, kv_ref=kv_ref, step=step):
                at = pl.multiple_of(i * step, step)
                kvs = [kv_ref[pl.ds(at, step), :]]
                return attend(qt_ref[...], kvs, head_dim, *carry, score_ref, weight_ref)

            state = lax.fori_loop(0, length // step, body, state)
    return state


def q_kernel(head_dim, tok_ref, wq_ref, gain_ref, table_ref, *refs):
    kv_refs = refs[:-6]
    qt_ref, top_ref, total_ref, acc_ref, *spare = refs[-6:]
    rows = tok_ref.shape[0]
    heads = wq_ref.shape[1] // head_dim
    raw = jnp.dot(tok_ref[...], wq_ref[...], preferred_element_type=jnp.float32)
    rounded = raw.astype(jnp.bfloat16)
    row_start = lax.axis_index("sp") * (rows // GRID_W)
    per = LANES // head_dim
    lane = lax.broadcasted_iota(jnp.int32, (1, LANES), 1)
    gain = jnp.concatenate([gain_ref[...]] * per, axis=1) * (head_dim ** -0.5)
    other_gain = swapped(gain, head_dim)
    swap = swap_matrix(head_dim)
    turns = []
    for j in range(rows // GRID_W):
        both = table_ref[0:GRID_W, :] + table_ref[pl.ds(GRID_W + row_start + j, 1), :]
        turns.append((gain * both[:, :LANES], other_gain * both[:, LANES:]))
    columns = []
    for p in range(heads // per):
        part = rounded[:, p * LANES : (p + 1) * LANES]
        other = jnp.dot(part, swap, preferred_element_type=jnp.float32)
        x = part.astype(jnp.float32)
        squares = x * x
        scale = None
        for g in range(per):
            mine = lane // head_dim == g
            mean = jnp.sum(jnp.where(mine, squares, 0.0), axis=1, keepdims=True) * (1.0 / head_dim)
            own = lax.rsqrt(mean + NORM_EPS)
            scale = own if scale is None else jnp.where(mine, own, scale)
        y = []
        for j, (cosine, sine) in enumerate(turns):
            some = slice(j * GRID_W, (j + 1) * GRID_W)
            y.append((x[some] * cosine + other[some] * sine) * scale[some])
        yt = jnp.concatenate(y, axis=0).T
        columns += [yt[g * head_dim : (g + 1) * head_dim] for g in range(per)]
    qt = jnp.concatenate(columns, axis=1)
    qt = jnp.concatenate([qt, jnp.zeros((LANES - head_dim, qt.shape[1]), jnp.float32)], axis=0)
    qt_ref[...] = qt.astype(jnp.bfloat16)
    state = attend_all(qt_ref, kv_refs, head_dim, (None, None, None), *spare)
    top_ref[...], total_ref[...], acc_ref[...] = state


def block_kernel(head_dim, qt_ref, *refs):
    kv_refs = refs[:-8]
    top_in, total_in, acc_in, top_ref, total_ref, acc_ref, *spare = refs[-8:]
    state = attend_all(qt_ref, kv_refs, head_dim, (top_in[...], total_in[...], acc_in[...]), *spare)
    top_ref[...], total_ref[...], acc_ref[...] = state


def finish_kernel(head_dim, qt_ref, *refs):
    kv_refs = refs[:-10]
    top_in, total_in, acc_in, wo_ref, att_ref, top_ref, sum_ref, sent_ref, *spare = refs[-10:]
    state = attend_all(qt_ref, kv_refs, head_dim, (top_in[...], total_in[...], acc_in[...]), *spare)
    top, total, acc = state
    summed = jnp.sum(total, axis=0, keepdims=True)
    out = acc * (1.0 / summed)
    rows = att_ref.shape[0]
    heads = top_ref.shape[0]
    per = LANES // head_dim
    for p in range(heads // per):
        pair = [out[:, h * rows : (h + 1) * rows] for h in range(p * per, (p + 1) * per)]
        att = jnp.concatenate(pair, axis=0).T
        att_ref[:, p * LANES : (p + 1) * LANES] = att.astype(jnp.bfloat16)
    own = sent_ref.shape[0]
    sent_ref[...] = product(att_ref, wo_ref, rows // own - 1, own).astype(jnp.bfloat16)
    for h in range(heads):
        top_ref[h : h + 1, :] = top[:, h * rows : (h + 1) * rows]
        sum_ref[h : h + 1, :] = summed[:, h * rows : (h + 1) * rows]


def product(att_ref, wo_ref, d, own):
    at = pl.multiple_of((lax.axis_index("tp") ^ d) * own, own)
    return jnp.dot(att_ref[pl.ds(at, own), :], wo_ref[...], preferred_element_type=jnp.float32)


def rest_kernel(att_ref, wo_ref, *out_refs):
    for d, out_ref in enumerate(out_refs):
        out = product(att_ref, wo_ref, d, out_ref.shape[0])
        out_ref[...] = out.astype(out_ref.dtype)


def call(kernel, out_shape, flops, in_specs, limit=LIMIT, **more):
    return pl.pallas_call(
        kernel,
        out_shape=out_shape,
        in_specs=in_specs,
        out_specs=jax.tree.map(lambda _: VMEM, out_shape),
        cost_estimate=pl.CostEstimate(flops=flops, bytes_accessed=flops // 256, transcendentals=0),
        compiler_params=pltpu.CompilerParams(vmem_limit_bytes=limit),
        **more,
    )


def xor(n, bit):
    return [(i, i ^ bit) for i in range(n)]


def shards(n_sp, n_tp, tokens, w_query, w_key, w_value, w_output, query_gain, key_gain):
    head_dim = query_gain.shape[0]
    rows, width = tokens.shape
    heads = w_query.shape[1] // head_dim
    table = rope_tables(n_sp * rows // GRID_W, head_dim)
    wide = jnp.asarray(np.pad(table, ((0, 0), (0, 7 * table.shape[1]))))
    table = jnp.asarray(table)
    f32 = functools.partial(jax.ShapeDtypeStruct, dtype=jnp.float32)
    bf16 = functools.partial(jax.ShapeDtypeStruct, dtype=jnp.bfloat16)
    pieces = 1

    scratch = [pltpu.VMEM((1, head_dim), jnp.float32), pltpu.VMEM((table.shape[0], 2 * LANES), jnp.float32)]
    kv = call(
        functools.partial(kv_kernel, head_dim),
        bf16((rows, LANES)),
        2 * rows * width * LANES,
        [HBM] * 3 + [VMEM, HBM],
        KV_LIMIT,
        scratch_shapes=[
            pltpu.VMEM(tokens.shape, jnp.bfloat16),
            pltpu.VMEM((LANES, width), jnp.bfloat16),
            scratch[1],
            pltpu.SemaphoreType.DMA((3 * pieces + 1,)),
        ],
    )(tokens, w_key.T, w_value.T, key_gain[None, :], wide)

    kv, tokens, w_query, w_output = lax.optimization_barrier((kv, tokens, w_query, w_output))
    size = heads * rows
    state_shape = [f32((1, size)), f32((8, size)), f32((head_dim, size))]

    def spare(kvs):
        count = min(SPAN, sum(x.shape[0] for x in kvs))
        return [pltpu.VMEM((count, size), jnp.float32), pltpu.VMEM((count, size), jnp.bfloat16)]

    def work(kvs):
        return sum(4 * size * x.shape[0] * LANES for x in kvs)

    def first(*kvs):
        qt, *state = call(
            functools.partial(q_kernel, head_dim),
            [bf16((LANES, size))] + state_shape,
            2 * rows * width * heads * head_dim + work(kvs),
            [VMEM] * (4 + len(kvs)),
            scratch_shapes=spare(kvs),
        )(tokens, w_query, query_gain[None, :], table, *kvs)
        return qt, state

    def blocks(qt, state, *kvs):
        return call(
            functools.partial(block_kernel, head_dim),
            state_shape,
            work(kvs),
            [VMEM] * (4 + len(kvs)),
            scratch_shapes=spare(kvs),
            input_output_aliases={1 + len(kvs) + i: i for i in range(3)},
        )(qt, *kvs, *state)

    own = rows // n_tp

    def finish(qt, state, *kvs):
        return call(
            functools.partial(finish_kernel, head_dim),
            [
                bf16((rows, heads * head_dim)),
                f32((heads, rows)),
                f32((heads, rows)),
                bf16((own, w_output.shape[1])),
            ],
            work(kvs),
            [VMEM] * (5 + len(kvs)),
            scratch_shapes=spare(kvs),
        )(qt, *kvs, *state, w_output)

    send = functools.partial(lax.ppermute, axis_name="sp")
    if n_sp == 8:
        near = send(kv, perm=xor(n_sp, 1))
        far = send(kv, perm=xor(n_sp, 4))
        pair = jnp.concatenate([kv, near], axis=0)
        middle = send(pair, perm=xor(n_sp, 6))
        beside = send(pair, perm=xor(n_sp, 2))
        relayed = send(far, perm=xor(n_sp, 1))
        qt, state = first(pair, beside, far)
        attended, top, summed, sent = finish(qt, state, relayed, middle)
    else:
        held = kv
        state = None
        stride = 1
        pending = [kv]
        while stride < n_sp:
            radix = 2 if stride == 1 else min(4, n_sp // stride)
            got = [send(held, perm=xor(n_sp, d * stride)) for d in range(1, radix)]
            if state is None:
                qt, state = first(*pending)
            else:
                state = blocks(qt, state, *pending)
            pending = got
            stride *= radix
            if stride < n_sp:
                held = jnp.concatenate([held] + got, axis=0)
        attended, top, summed, sent = finish(qt, state, *pending)

    parts = call(
        rest_kernel,
        [(bf16 if d % 2 else f32)(sent.shape) for d in range(n_tp - 1)],
        2 * rows * w_output.size // n_tp,
        [VMEM] * 2,
    )(attended, w_output)
    parts = [*parts, sent]
    bit = 1
    while bit < n_tp:
        for d in reversed(range(0, n_tp, 2 * bit)):
            got = lax.ppermute(parts[d + bit].astype(jnp.bfloat16), "tp", xor(n_tp, bit))
            parts[d] = parts[d] + got.astype(jnp.float32)
        bit *= 2
    return parts[0].astype(jnp.bfloat16), top + jnp.log(summed)


def solution(mesh):
    placed = (P("sp", None), P(None, "tp"), P(None, "tp"), P(None, "tp"), P("tp", None), P(), P())
    return jax.shard_map(
        functools.partial(shards, mesh.shape["sp"], mesh.shape["tp"]),
        mesh=mesh,
        in_specs=placed,
        out_specs=(P(("sp", "tp"), None), P("tp", "sp")),
        check_vma=False,
    )
```
